32 devices in a mesh: ep: 8 (over z, core), tp: 4 (over y, x).
Axes of the slice: x: 2, y: 2, z: 4, core: 2. Of those that a mesh axis runs over, the one named last changes fastest.
Arguments:
- tokens: bfloat16 [1024, 2048], P('ep'), may hold values from -6 to 6
- cotangent: bfloat16 [1024, 2048], P('ep'), may hold values from -6 to 6
- expert_ids: int32 [1024, 2], P('ep'), may hold values from 0 to 7, all different within a row; in each aligned block of 128 rows (0 to 127, 128 to 255, ...) at most 64 rows name the same one
- route_weight: bfloat16 [1024, 2], P('ep'), may hold values from 0.19921875 to 1
- gate_weight: bfloat16 [8, 1024, 2048], P('ep', 'tp'), may hold values from -0.125 to 0.125
- up_weight: bfloat16 [8, 1024, 2048], P('ep', 'tp'), may hold values from -0.125 to 0.125
- down_weight: bfloat16 [8, 1024, 2048], P('ep', 'tp'), may hold values from -0.1875 to 0.1875
Outputs:
- tokens_grad: bfloat16 [1024, 2048], P('ep', 'tp')
- route_weight_grad: float32 [1024, 2], P('ep')
- gate_weight_grad: float32 [8, 1024, 2048], P('ep', 'tp')
- up_weight_grad: float32 [8, 1024, 2048], P('ep', 'tp')
- down_weight_grad: float32 [8, 1024, 2048], P('ep', 'tp')
The draws below stay inside these ranges and needn't reach their ends.
Inputs may be any that keep to these rules, and one draw needn't show every extreme that they name: `expert_ids`: within each aligned block of 128 rows every expert is named at most 64 times; the two experts of a row differ.
All inputs are finite; a program needn't handle non-finite values.
Results may differ from the reference program's by a relative error of at most 0.0058.
Values may be sent and summed in bfloat16 or wider, within the bound.
A program may use at most 64 MiB of HBM per device.

```python
import math
import jax
import jax.numpy as jnp
import numpy as np
from jax import lax

D = 2048
FE = 1024
TOP = 2
TOK_DEV = 128
EXPERTS = 8
TOKENS = 1024
CAP = 64
N_EP = 8


def block_scale(rng, shape, split, smallest, high):
    loudness, own = 1.0, jax.random.fold_in(rng, 6)
    for axis_at, parts in split:
        draws = jnp.exp(jax.random.uniform(jax.random.fold_in(own, axis_at), (parts,), jnp.float32, smallest / len(split), high / len(split)))
        loudness = loudness * jnp.repeat(draws, shape[axis_at] // parts).reshape([-1 if axis == axis_at else 1 for axis in range(len(shape))])
    return loudness


def assign_block(own_key, own, number, rows, count, top, most, slope):
    sequence = jax.random.permutation(own_key, count)
    crowded, common = load_shares(count, rows * top, most, slope, True), load_shares(count, rows * top, most, slope, False)
    places = jnp.arange(count)

    def named(tallies, turn):
        used = int((tallies > 0).sum())
        fixed = max(1, used // 4)
        shifted = fixed + (places - fixed + turn * (used - fixed)) % max(1, count - fixed)
        return jnp.zeros((count,), jnp.int32).at[sequence[jnp.where(places < fixed, places, shifted)]].set(jnp.asarray(tallies, jnp.int32))

    tallies = jnp.where(number % 4 == 0, named(crowded, number // 4), named(common, number - number // 4 - 1))
    mixed = jax.random.permutation(jax.random.fold_in(own, 3), count)
    source_of, taker = mixed[0:count // 2 * 2:2], mixed[1:count // 2 * 2:2]
    slack = jnp.minimum(tallies[source_of] - 1, most - tallies[taker]) // 2
    slack = jnp.where((source_of == sequence[0]) | (taker == sequence[0]) | (tallies[taker] == 0), 0, jnp.maximum(slack, 0))
    shifted = jax.random.randint(jax.random.fold_in(own, 4), (count // 2,), 0, 1 << 20) % (slack + 1)
    tallies = tallies.at[source_of].add(-shifted).at[taker].add(shifted)
    items = jnp.searchsorted(jnp.cumsum(tallies), jnp.arange(rows * top), side="right").astype(jnp.int32)
    listing = items.reshape(top, rows).T
    listing = listing[jax.random.permutation(jax.random.fold_in(own, 1), rows)]
    turn = jax.random.randint(jax.random.fold_in(own, 2), (rows, 1), 0, top)
    return jnp.take_along_axis(listing, (jnp.arange(top)[None, :] + turn) % top, axis=1)


def load_shares(amount, total, most, slope, full):
    portions = [(1 << 20) // math.isqrt(rank ** slope) + 1 for rank in range(1, amount + 1)]
    largest = most if full else min(most, max(-(-total // amount), total * portions[0] // sum(portions)))
    least = 1 if total - largest >= amount - 1 else 0
    given, spare = [largest] + [least] * (amount - 1), total - largest - least * (amount - 1)
    while spare > 0:
        free = [i for i in range(1, amount) if given[i] < largest] or [i for i in range(1, amount) if given[i] < most]
        whole, left = sum([portions[i] for i in free]), spare
        for i in free:
            extra = min(most - given[i], max(1, left * portions[i] // whole), spare)
            given[i] = given[i] + extra
            spare = spare - extra
    return np.array(given)


def gaussian(stream_key, shape, spread, reach, cuts=(), kind=jnp.bfloat16):
    entries = spread * jax.random.normal(stream_key, shape, jnp.float32)
    if cuts:
        entries = entries * block_scale(stream_key, shape, cuts, -0.22, 0.18)
    return jnp.clip(entries, -reach, reach).astype(kind)


def setup_inputs(seed: int = 0) -> dict:
    streams_of = jax.random.split(jax.random.key(seed), 8)
    tokens = gaussian(streams_of[0], (TOKENS, D), 1.0, 6.0, ((0, 8),))
    cotangent = gaussian(streams_of[1], (TOKENS, D), 1.0, 6.0, ((0, 8),))
    expert_ids_keys = jax.random.split(jax.random.fold_in(streams_of[2], 1), TOKENS // TOK_DEV)
    expert_ids_turns = jax.random.permutation(jax.random.fold_in(streams_of[2], 3), TOKENS // TOK_DEV)
    expert_ids = jax.vmap(lambda own, number: assign_block(jax.random.fold_in(streams_of[2], 2), own, number, TOK_DEV, EXPERTS, TOP, CAP, 2))(expert_ids_keys, expert_ids_turns).reshape((TOKENS, TOP))
    route_weight = jnp.clip(0.19921875 + 0.80078125 * jax.random.uniform(streams_of[3], (TOKENS, TOP), jnp.float32) ** block_scale(streams_of[3], (TOKENS, TOP), ((0, 8),), -0.2, 0.2), 0.19921875, 1.0).astype(jnp.bfloat16)
    gate_weight = gaussian(streams_of[4], (EXPERTS, FE, D), D ** -0.5, 0.125, ((0, 8), (1, 4)))
    up_weight = gaussian(streams_of[5], (EXPERTS, FE, D), D ** -0.5, 0.125, ((0, 8), (1, 4)))
    down_weight = gaussian(streams_of[6], (EXPERTS, FE, D), FE ** -0.5, 0.1875, ((0, 8), (1, 4)))
    return {"tokens": tokens, "cotangent": cotangent, "expert_ids": expert_ids, "route_weight": route_weight, "gate_weight": gate_weight, "up_weight": up_weight, "down_weight": down_weight}


def reference(tokens, cotangent, expert_ids, route_weight, gate_weight, up_weight, down_weight):
    routed = TOKENS * TOP
    buffer_rows = N_EP * CAP
    flat_ids = expert_ids.reshape(-1)
    flat_weight = route_weight.reshape(-1)

    def one_expert(expert):
        picked = jnp.nonzero(flat_ids == expert, size=buffer_rows, fill_value=routed)[0].astype(jnp.int32)
        usable = picked < routed
        safe_pair = jnp.minimum(picked, routed - 1)
        token_of = safe_pair // TOP
        routed_rows = tokens[token_of]
        routed_cotangent = cotangent[token_of]
        weight = jnp.where(usable, flat_weight[safe_pair].astype(jnp.float32), jnp.float32(0.0))[:, None]
        gate_w = lax.dynamic_index_in_dim(gate_weight, expert, 0, keepdims=False)
        up_w = lax.dynamic_index_in_dim(up_weight, expert, 0, keepdims=False)
        down_w = lax.dynamic_index_in_dim(down_weight, expert, 0, keepdims=False)
        pre_gate = jnp.dot(routed_rows, gate_w.T, preferred_element_type=jnp.float32)
        pre_up = jnp.dot(routed_rows, up_w.T, preferred_element_type=jnp.float32)
        sigma = jax.nn.sigmoid(pre_gate)
        silu_gate = pre_gate * sigma
        hidden = silu_gate * pre_up
        back_hidden = jnp.dot(routed_cotangent, down_w.T, preferred_element_type=jnp.float32)
        products = jnp.sum(hidden * back_hidden, axis=1)
        scaled = weight * back_hidden
        grad_gate = (scaled * pre_up * sigma * (1.0 + pre_gate * (1.0 - sigma))).astype(jnp.bfloat16)
        grad_up = (scaled * silu_gate).astype(jnp.bfloat16)
        weighted = (weight * hidden).astype(jnp.bfloat16)
        down_grad = jnp.dot(weighted.T, routed_cotangent, preferred_element_type=jnp.float32)
        gate_grad = jnp.dot(grad_gate.T, routed_rows, preferred_element_type=jnp.float32)
        up_grad = jnp.dot(grad_up.T, routed_rows, preferred_element_type=jnp.float32)
        pair_grad = (jnp.dot(grad_gate, gate_w, preferred_element_type=jnp.float32)
                     + jnp.dot(grad_up, up_w, preferred_element_type=jnp.float32)).astype(jnp.bfloat16)
        return gate_grad, up_grad, down_grad, picked, pair_grad, products

    gate_grad, up_grad, down_grad, picked, pair_grad, products = lax.map(
        one_expert, jnp.arange(EXPERTS, dtype=jnp.int32))
    slot_flat = picked.reshape(-1)
    token_sum = jnp.zeros((routed, D), jnp.float32).at[slot_flat].set(
        pair_grad.reshape(-1, D).astype(jnp.float32), mode="drop")
    tokens_grad = jnp.sum(token_sum.reshape(TOKENS, TOP, D), axis=1).astype(jnp.bfloat16)
    route_grad = jnp.zeros((routed,), jnp.float32).at[slot_flat].set(products.reshape(-1), mode="drop")
    return tokens_grad, route_grad.reshape(TOKENS, TOP), gate_grad, up_grad, down_grad
```

```python
import functools

import jax
import jax.numpy as jnp
from jax import lax
from jax.experimental import pallas as pl
from jax.experimental.pallas import tpu as pltpu
from jax.sharding import PartitionSpec as P

MESH = pl.DeviceIdType.MESH
F32 = jnp.float32
BF16 = jnp.bfloat16


def slices_for(j, tp, bits, count):
    base = j
    for bit in bits:
        base = base - ((j // bit) % 2) * bit
    out = []
    for k in range(count):
        out.append(base + sum(bit for n, bit in enumerate(bits) if (k >> n) & 1))
    return out


def kernel(
    ep, tp, tokens, cotangent, ids, probs, gate_w, up_w, down_w,
    dx_out, route_out, gate_out, up_out, down_out,
    rows, weights, pair_w, wg, part, core_in, tp_in, z_in, grads, r_send, r_in, r_tp,
    load_sem, wz_send, wz_recv, z_send, z_recv, t_send, t_recv, c_send, c_recv,
    pc_send, pc_recv, pt_send, pt_recv, pz_send, pz_recv, rs_send, rs_recv, rt_send, rt_recv,
):
    e, j = lax.axis_index("ep"), lax.axis_index("tp")
    levels = ep // 2
    lvl, core = e // 2, e % 2
    t_rows, width = tokens.shape
    span = width // tp
    half = t_rows // 2
    f_rows = gate_w.shape[0]
    nb = tp.bit_length() - 1
    slots = part.shape[0]
    mate = 2 * lvl + 1 - core

    def order(i):
        near = jnp.minimum(lvl, levels - 1 - lvl)
        d = (i + 1) // 2
        close = jnp.where(i % 2 == 1, lvl - d, lvl + d)
        far = jnp.where(lvl == near, lvl + (i - near), lvl - (i - near))
        return jnp.where(i <= 2 * near, close, far)

    def row0(l, c):
        return pl.multiple_of((2 * l + c) * t_rows, t_rows)

    def col(s):
        return pl.ds(pl.multiple_of(s * span, span), span)

    def flip(bit):
        return j + bit * (1 - 2 * ((j // bit) % 2))

    def remote(src, dst, ssem, rsem, de, dt):
        return pltpu.make_async_remote_copy(
            src_ref=src, dst_ref=dst, send_sem=ssem, recv_sem=rsem,
            device_id=(de, dt), device_id_type=MESH)

    own = pl.ds(row0(lvl, core), t_rows)
    loads = [
        pltpu.make_async_copy(tokens, rows.at[0, own], load_sem.at[0]),
        pltpu.make_async_copy(cotangent, rows.at[1, own], load_sem.at[1]),
        pltpu.make_async_copy(gate_w, weights.at[0], load_sem.at[2]),
        pltpu.make_async_copy(up_w, weights.at[1], load_sem.at[3]),
        pltpu.make_async_copy(down_w, weights.at[2], load_sem.at[4]),
    ]
    for copy in loads:
        copy.start()
    barrier = pltpu.get_barrier_semaphore()

    def greet(n, _):
        pl.semaphore_signal(barrier, inc=1, device_id=(lax.rem(e + n, ep), j), device_id_type=MESH)
        return 0

    def greet_tp(n, _):
        pl.semaphore_signal(barrier, inc=1, device_id=(e, lax.rem(j + n, tp)), device_id_type=MESH)
        return 0

    lax.fori_loop(1, ep, greet, 0)
    lax.fori_loop(1, tp, greet_tp, 0)
    pl.semaphore_wait(barrier, ep + tp - 2)

    def w_copy(d):
        return remote(pair_w.at[d], wg.at[e], wz_send.at[d], wz_recv.at[e], d, j)

    def w_wait(src):
        return remote(pair_w.at[src], wg.at[src], wz_send.at[src], wz_recv.at[src], src, j)

    def z_copy(a, l, side):
        ref = rows.at[a, pl.ds(row0(l, core), t_rows), col(j)]
        de = lax.rem(e + (2 if side else ep - 2), ep)
        return remote(ref, ref, z_send.at[a, side, l], z_recv.at[a, l], de, j)

    def gather_step(a, l, s, receive):
        copies = []
        for h in range(2):
            order_bits = [1 << b for b in (range(nb) if h == 0 else range(nb - 1, -1, -1))]
            peer = flip(order_bits[s])
            ids = slices_for(peer if receive else j, tp, order_bits[:s], 1 << s)
            for k, sid in enumerate(ids):
                ref = rows.at[a, pl.ds(row0(l, core) + h * half, half), col(sid)]
                copies.append(remote(
                    ref, ref, t_send.at[a, l, h, (1 << s) - 1 + k], t_recv.at[a, l, h, sid], e, peer))
        return copies

    def core_copy(a, l, c):
        ref = rows.at[a, pl.ds(row0(l, c), t_rows)]
        return remote(ref, ref, c_send.at[a, l], c_recv.at[a, l], mate, j)

    def pc_copy(l, i):
        return remote(part.at[i % slots, 1 - core], core_in.at[l], pc_send.at[l], pc_recv.at[l], mate, j)

    def scatter_step(l, i, s, receive):
        copies = []
        base = sum(tp >> (n + 1) for n in range(s))
        count = tp >> (s + 1)
        for h in range(2):
            order_bits = [1 << b for b in (range(nb) if h == 0 else range(nb - 1, -1, -1))]
            peer = flip(order_bits[s])
            ids = slices_for(j if receive else peer, tp, order_bits[s + 1:], count)
            for k, sid in enumerate(ids):
                src = part.at[i % slots, core, pl.ds(h * half, half), col(sid)]
                dst = tp_in.at[l, h, base + k]
                copies.append((remote(src, dst, pt_send.at[l, h, base + k], pt_recv.at[l, h, base + k], e, peer),
                               src, dst))
        return copies

    def pz_copy(l, i):
        return remote(part.at[i % slots, core, :, col(j)], z_in.at[lvl], pz_send.at[l], pz_recv.at[lvl],
                      2 * l + core, j)

    def pz_wait(src):
        return remote(part.at[0, core, :, col(j)], z_in.at[src], pz_send.at[src], pz_recv.at[src],
                      2 * src + core, j)

    def pair_row(d, _):
        pair_w[d] = jnp.sum(
            jnp.where(ids[...] == d, probs[...].astype(F32), 0.0), axis=0, keepdims=True)
        return 0

    for n in range(2):
        loads[n].wait()
        @pl.when(lvl + 1 < levels)
        def _():
            z_copy(n, lvl, 1).start()
        @pl.when(lvl > 0)
        def _():
            z_copy(n, lvl, 0).start()
        core_copy(n, lvl, core).start()

    lax.fori_loop(0, ep, pair_row, 0)

    def w_start(n, _):
        w_copy(lax.rem(e + n, ep)).start()
        return 0

    lax.fori_loop(1, ep, w_start, 0)
    wg[e] = pair_w[e]
    for n in range(2, 5):
        loads[n].wait()

    def arrive(i):
        l = order(i)
        for a in range(2):
            z_copy(a, l, 0).wait_recv()
            @pl.when(jnp.logical_and(l < lvl, lvl + 1 < levels))
            def _():
                z_copy(a, l, 1).start()
            @pl.when(jnp.logical_and(l > lvl, lvl > 0))
            def _():
                z_copy(a, l, 0).start()
            for copy in gather_step(a, l, 0, False):
                copy.start()

    def spread(i, s):
        l = order(i)
        for a in range(2):
            for copy in gather_step(a, l, s - 1, True):
                copy.wait_recv()
            if s < nb:
                for copy in gather_step(a, l, s, False):
                    copy.start()
            else:
                core_copy(a, l, core).start()

    def compute(i):
        l = order(i)
        for a in range(2):
            core_copy(a, l, 1 - core).wait_recv()
        @pl.when(l != lvl)
        def _():
            w_wait(2 * l).wait_recv()
            w_wait(2 * l + 1).wait_recv()
        @pl.when(l == lvl)
        def _():
            w_wait(mate).wait_recv()
        sel = pl.ds(row0(l, 0), 2 * t_rows)
        nt = (((1,), (1,)), ((), ()))
        x = rows[0, sel, :]
        pre_gate = lax.dot_general(weights[0], x, nt, preferred_element_type=F32)
        pre_up = lax.dot_general(weights[1], x, nt, preferred_element_type=F32)
        back = lax.dot_general(weights[2], rows[1, sel, :], nt, preferred_element_type=F32)
        p = jnp.concatenate([wg[2 * l], wg[2 * l + 1]], axis=1)
        sigma = jax.nn.sigmoid(pre_gate)
        silu = pre_gate * sigma
        hidden = silu * pre_up
        prod = jnp.sum(hidden * back, axis=0, keepdims=True)
        r_send[2 * l] = prod[:, :t_rows]
        r_send[2 * l + 1] = prod[:, t_rows:]
        scaled = p * back
        gg = (scaled * pre_up * sigma * (1.0 + pre_gate * (1.0 - sigma))).astype(BF16)
        gu = (scaled * silu).astype(BF16)
        grads[0, :, sel] = gg
        grads[1, :, sel] = gu
        grads[2, :, sel] = (p * hidden).astype(BF16)
        ggt, gut = gg.T, gu.T
        tile = min(width, 512)

        def column(n, _):
            cs = pl.ds(pl.multiple_of(n * tile, tile), tile)
            d = (jnp.dot(ggt, weights[0, :, cs], preferred_element_type=F32)
                 + jnp.dot(gut, weights[1, :, cs], preferred_element_type=F32)).astype(BF16)
            part[i % slots, 0, :, cs] = d[:t_rows]
            part[i % slots, 1, :, cs] = d[t_rows:]
            return 0

        lax.fori_loop(0, width // tile, column, 0)
        pc_copy(l, i).start()

        def send_r(d):
            remote(r_send.at[d], r_in.at[e], rs_send.at[d], rs_recv.at[e], d, j).start()
        for c in range(2):
            @pl.when(2 * l + c != e)
            def _():
                send_r(2 * l + c)
            @pl.when(2 * l + c == e)
            def _():
                r_in[2 * l + c] = r_send[2 * l + c]

    def merge_core(i):
        l = order(i)
        pc_copy(l, i).wait()
        part[i % slots, core] = (part[i % slots, core].astype(F32) + core_in[l].astype(F32)).astype(BF16)
        for copy, _, _ in scatter_step(l, i, 0, False):
            copy.start()

    def merge_tp(i, s):
        l = order(i)
        for (copy, _, _), (_, mine, got) in zip(scatter_step(l, i, s, False), scatter_step(l, i, s, True)):
            copy.wait()
            mine[...] = (mine[...].astype(F32) + got[...].astype(F32)).astype(BF16)
        if s + 1 < nb:
            for copy, _, _ in scatter_step(l, i, s + 1, False):
                copy.start()
        else:
            @pl.when(l != lvl)
            def _():
                pz_copy(l, i).start()
            @pl.when(l == lvl)
            def _():
                z_in[lvl] = part[i % slots, core, :, col(j)]

    def drain(i):
        l = order(i)
        @pl.when(l != lvl)
        def _():
            pz_copy(l, i).wait_send()

    outs = (gate_out, up_out, down_out)

    def weight_grad(k):
        tile = min(width, 512)

        def column(n, _):
            cs = pl.ds(pl.multiple_of(n * tile, tile), tile)
            outs[k][:, cs] = jnp.dot(
                grads[k], rows[k // 2, :, cs], preferred_element_type=F32)
            return 0

        lax.fori_loop(0, width // tile, column, 0)

    compute(0)
    d_comp = nb + 1
    last = levels - 1 + d_comp

    def tick(t, _):
        def stage(f, i, low):
            @pl.when(jnp.logical_and(i >= low, i < levels))
            def _():
                f(i)
        def back(late):
            return jnp.where(t == 1 + late, 0, jnp.where(t > d_comp + late, t - d_comp - late, -1))

        for k in range(3):
            @pl.when(t == last + k)
            def _():
                weight_grad(k)
        stage(drain, back(nb + 1), 0)
        for s in range(nb, 0, -1):
            stage(functools.partial(spread, s=s), t - s, 1)
        stage(arrive, t, 1)
        for s in range(nb - 1, -1, -1):
            stage(functools.partial(merge_tp, s=s), back(1 + s), 0)
        stage(compute, t - d_comp + 1, 1)
        stage(merge_core, back(0), 0)
        return 0

    lax.fori_loop(1, levels + d_comp + nb + 1, tick, 0)

    def r_wait(n, _):
        src = lax.rem(e + n, ep)
        remote(r_send.at[src], r_in.at[src], rs_send.at[src], rs_recv.at[src], src, j).wait()
        return 0

    lax.fori_loop(1, ep, r_wait, 0)

    def rt_copy(n):
        dt = lax.rem(j + n, tp)
        return remote(r_in, r_tp.at[j], rt_send.at[dt], rt_recv.at[j], e, dt)

    def rt_wait(n, _):
        src = lax.rem(j + n, tp)
        remote(r_in, r_tp.at[src], rt_send.at[src], rt_recv.at[src], e, src).wait()
        return 0

    def rt_start(n, _):
        rt_copy(n).start()
        return 0

    lax.fori_loop(1, tp, rt_start, 0)
    r_tp[j] = r_in[...]

    def pz_drain(src, _):
        @pl.when(src != lvl)
        def _():
            pz_wait(src).wait_recv()
        return 0

    lax.fori_loop(0, levels, pz_drain, 0)
    dx_out[...] = jnp.sum(z_in[...].astype(F32), axis=0).astype(BF16)
    lax.fori_loop(1, tp, rt_wait, 0)
    r_in[...] = jnp.sum(r_tp[...], axis=0)

    def choose(d, acc):
        return acc + jnp.where(ids[...] == d, r_in[d], 0.0)

    route_out[...] = lax.fori_loop(0, ep, choose, jnp.zeros(route_out.shape, F32))

    for a in range(2):
        @pl.when(lvl + 1 < levels)
        def _():
            z_copy(a, lvl, 1).wait_send()
        @pl.when(lvl > 0)
        def _():
            z_copy(a, lvl, 0).wait_send()

    def finish(l, _):
        for a in range(2):
            core_copy(a, l, core).wait_send()
            @pl.when(jnp.logical_and(l < lvl, lvl + 1 < levels))
            def _():
                z_copy(a, l, 1).wait_send()
            @pl.when(jnp.logical_and(l > lvl, lvl > 0))
            def _():
                z_copy(a, l, 0).wait_send()
            @pl.when(l != lvl)
            def _():
                for s in range(nb):
                    for copy in gather_step(a, l, s, False):
                        copy.wait_send()
        return 0

    lax.fori_loop(0, levels, finish, 0)

    def w_done(n, _):
        w_copy(lax.rem(e + n, ep)).wait_send()
        return 0

    lax.fori_loop(1, ep, w_done, 0)


def publish(*refs):
    srcs, dsts, sem = refs[:5], refs[5:10], refs[10]
    copies = [pltpu.make_async_copy(srcs[k], dsts[k], sem.at[k]) for k in (2, 3, 4, 0, 1)]
    for copy in copies:
        copy.start()
    for copy in copies:
        copy.wait()


def per_device(tokens, cotangent, expert_ids, route_weight, gate_weight, up_weight, down_weight):
    ep, tp = lax.axis_size("ep"), lax.axis_size("tp")
    t_rows, width = tokens.shape
    _, f_rows, _ = gate_weight.shape
    levels = ep // 2
    span = width // tp
    slots = min(levels, 8)
    any_, vmem = pl.BlockSpec(memory_space=pl.ANY), pl.BlockSpec(memory_space=pltpu.VMEM)
    dma = pltpu.SemaphoreType.DMA
    big = pltpu.VMEM((f_rows, width), F32)
    scratch = [
        pltpu.VMEM((2, ep * t_rows, width), BF16),
        pltpu.VMEM((3, f_rows, width), BF16),
        pltpu.VMEM((ep, 1, t_rows), F32),
        pltpu.VMEM((ep, 1, t_rows), F32),
        pltpu.VMEM((slots, 2, t_rows, width), BF16),
        pltpu.VMEM((levels, t_rows, width), BF16),
        pltpu.VMEM((levels, 2, tp - 1, t_rows // 2, span), BF16),
        pltpu.VMEM((levels, t_rows, span), BF16),
        pltpu.VMEM((3, f_rows, ep * t_rows), BF16),
        pltpu.VMEM((ep, 1, t_rows), F32),
        pltpu.VMEM((ep, 1, t_rows), F32),
        pltpu.VMEM((tp, ep, 1, t_rows), F32),
        dma((5,)), dma((ep,)), dma((ep,)), dma((2, 2, levels)), dma((2, levels)),
        dma((2, levels, 2, tp - 1)), dma((2, levels, 2, tp)), dma((2, levels)), dma((2, levels)),
        dma((levels,)), dma((levels,)), dma((levels, 2, tp - 1)), dma((levels, 2, tp - 1)),
        dma((levels,)), dma((levels,)), dma((ep,)), dma((ep,)), dma((tp,)), dma((tp,)),
    ]
    dx, route, gate_grad, up_grad, down_grad = pl.pallas_call(
        functools.partial(kernel, ep, tp),
        out_shape=(
            pltpu.VMEM((t_rows, span), BF16),
            pltpu.VMEM(expert_ids.shape[::-1], F32), big, big, big),
        in_specs=[any_, any_, vmem, vmem, any_, any_, any_],
        out_specs=(vmem, vmem, vmem, vmem, vmem),
        scratch_shapes=scratch,
        compiler_params=pltpu.CompilerParams(
            collective_id=0, has_side_effects=True, vmem_limit_bytes=66_900_000 - 12 * f_rows * width - 2 * t_rows * span),
    )(tokens, cotangent, expert_ids.T, route_weight.T, gate_weight[0], up_weight[0], down_weight[0])
    pieces = (dx, route, gate_grad, up_grad, down_grad)
    dx, route, *wide = pl.pallas_call(
        publish,
        out_shape=tuple(jax.ShapeDtypeStruct(v.shape, v.dtype) for v in pieces),
        in_specs=[vmem] * 5,
        out_specs=(any_,) * 5,
        scratch_shapes=[dma((5,))],
        compiler_params=pltpu.CompilerParams(vmem_limit_bytes=1_000_000),
    )(*(pltpu.with_memory_space_constraint(v, pltpu.VMEM) for v in pieces))
    return dx, route.T, *(g[None] for g in wide)


def solution(mesh):
    in_specs = (
        P("ep", None), P("ep", None), P("ep", None), P("ep", None),
        P("ep", "tp", None), P("ep", "tp", None), P("ep", "tp", None),
    )
    out_specs = (
        P("ep", "tp"), P("ep", None), P("ep", "tp", None), P("ep", "tp", None), P("ep", "tp", None),
    )
    return jax.shard_map(
        per_device, mesh=mesh, in_specs=in_specs, out_specs=out_specs, check_vma=False
    )
```

```python
import functools

import jax
import jax.numpy as jnp
from jax import lax
from jax.experimental import pallas as pl
from jax.experimental.pallas import tpu as pltpu
from jax.sharding import PartitionSpec as P

MESH = pl.DeviceIdType.MESH
F32 = jnp.float32
BF16 = jnp.bfloat16
NT = (((1,), (1,)), ((), ()))
TN = (((0,), (0,)), ((), ()))
VMEM_BYTES = 66_900_000
AHEAD = 1


def slices_for(j, bits, count):
    base = j
    for bit in bits:
        base = base - ((j // bit) % 2) * bit
    out = []
    for k in range(count):
        out.append(base + sum(bit for n, bit in enumerate(bits) if (k >> n) & 1))
    return out


def kernel(
    ep, tp, cap, tokens, cotangent, ids_in, probs_in, gate_w, up_w, down_w,
    dx_out, route_out, gate_out, up_out, down_out,
    ids, probs, xin, hot, hot_t, stage, mate_rows, whole, rows, weights, pw_out, pw_in, grads, part, ta_in, tb_in, z_in,
    r_send, r_in, r_tp, r_mat,
    load_sem, z_send, z_recv, m_send, m_recv, f_send, f_recv, w_send, w_recv, ta_send, ta_recv, tb_send, tb_recv,
    pa_send, pa_recv, pb_send, pb_recv, pz_send, pz_recv, rs_send, rs_recv, rt_send, rt_recv,
):
    e, j = lax.axis_index("ep"), lax.axis_index("tp")
    levels = ep // 2
    lvl, core = e // 2, e % 2
    mate = e + 1 - 2 * core
    t_rows, width = tokens.shape
    span = width // tp
    half = cap // 2
    nb = tp.bit_length() - 1
    lb = levels.bit_length() - 1
    far = 2 * (levels - 1)
    units = far + 2
    tile = min(width, 512)

    def xor(a, b):
        out = 0
        for n in range(lb):
            p, q = (a // (1 << n)) % 2, (b // (1 << n)) % 2
            out = out + (p + q - 2 * p * q) * (1 << n)
        return out

    def level_of(u):
        d = u // 2 + 1 + u % 2
        return xor(lvl, jnp.where(d >= levels, 1, d))

    def source(v):
        u = jnp.maximum(v - 2, 0)
        return jnp.where(v == 0, e, jnp.where(v == 1, mate, 2 * level_of(u) + u % 2))

    def blk(s):
        return pl.ds(pl.multiple_of(s * cap, cap), cap)

    def col(s):
        return pl.ds(pl.multiple_of(s * span, span), span)

    def run(first, count):
        return pl.ds(pl.multiple_of(first * span, span), count * span)

    def flip(bit):
        return j + bit * (1 - 2 * ((j // bit) % 2))

    def remote(src, dst, ssem, rsem, de, dt):
        return pltpu.make_async_remote_copy(
            src_ref=src, dst_ref=dst, send_sem=ssem, recv_sem=rsem,
            device_id=(de, dt), device_id_type=MESH)

    small = [
        pltpu.make_async_copy(ids_in, ids, load_sem.at[5]),
        pltpu.make_async_copy(probs_in, probs, load_sem.at[6]),
    ]
    loads = [
        pltpu.make_async_copy(tokens, xin.at[0], load_sem.at[0]),
        pltpu.make_async_copy(cotangent, xin.at[1], load_sem.at[1]),
        pltpu.make_async_copy(gate_w, weights.at[0], load_sem.at[2]),
        pltpu.make_async_copy(up_w, weights.at[1], load_sem.at[3]),
        pltpu.make_async_copy(down_w, weights.at[2], load_sem.at[4]),
    ]
    for copy in small + loads:
        copy.start()
    barrier = pltpu.get_barrier_semaphore()

    def greet(n, _):
        pl.semaphore_signal(barrier, inc=1, device_id=(lax.rem(e + n, ep), j), device_id_type=MESH)
        return 0

    def greet_tp(n, _):
        pl.semaphore_signal(barrier, inc=1, device_id=(e, lax.rem(j + n, tp)), device_id_type=MESH)
        return 0

    lax.fori_loop(1, ep, greet, 0)
    lax.fori_loop(1, tp, greet_tp, 0)

    def z_copy(a, d):
        return remote(stage.at[a, blk(d)], rows.at[a, blk(e), col(j)],
                      z_send.at[a, d], z_recv.at[a, e], d, j)

    def z_wait(a, s):
        return remote(stage.at[a, blk(s)], rows.at[a, blk(s), col(j)],
                      z_send.at[a, s], z_recv.at[a, s], s, j)

    def m_copy(a, s):
        return remote(mate_rows.at[a], rows.at[a, blk(s)], m_send.at[a], m_recv.at[a], mate, j)

    def full_copy(a, c, s, d):
        return remote(whole.at[a, c], rows.at[a, blk(s)], f_send.at[a, c], f_recv.at[a], d, j)

    def w_copy(d, s):
        return remote(pw_out.at[d], pw_in.at[s], w_send.at[d], w_recv.at[s], d, j)

    def gather_step(a, s, n, receive):
        peer = flip(1 << n if a == 0 else tp >> (n + 1))
        owner = peer if receive else j
        if a == 0:
            ref = rows.at[a, blk(s), run(owner - owner % (1 << n), 1 << n)]
            return [remote(ref, ref, ta_send.at[s, n], ta_recv.at[s, n], e, peer)]
        copies = []
        for k, sid in enumerate(slices_for(owner, [tp >> (i + 1) for i in range(n)], 1 << n)):
            ref = rows.at[a, blk(s), col(sid)]
            at = (1 << n) - 1 + k
            copies.append(remote(ref, ref, tb_send.at[s, at], tb_recv.at[s, at], e, peer))
        return copies

    def scatter_step(s, n, receive):
        base, count = tp - (tp >> n), tp >> (n + 1)
        copies = []
        peer = flip(1 << n)
        owner = j if receive else peer
        for k, sid in enumerate(slices_for(owner, [1 << i for i in range(n + 1, nb)], count)):
            src, dst, at = part.at[s, :half, col(sid)], tb_in.at[s, base + k], base + k
            copies.append((remote(src, dst, pb_send.at[s, at], pb_recv.at[s, at], e, peer), src, dst))
        peer = flip(count)
        owner = j if receive else peer
        src = part.at[s, half:, run(owner - owner % count, count)]
        dst = ta_in.at[s, :, base * span:(base + count) * span]
        copies.append((remote(src, dst, pa_send.at[s, n], pa_recv.at[s, n], e, peer), src, dst))
        return copies

    def pz_copy(d, s):
        return remote(part.at[d, :, col(j)], z_in.at[blk(s)], pz_send.at[d], pz_recv.at[s], d, j)

    def r_copy(d, s):
        return remote(r_send.at[d], r_in.at[s], rs_send.at[d], rs_recv.at[s], d, j)

    def send(u, arrays):
        l = level_of(u)
        for a in arrays:
            for c in range(2):
                z_copy(a, 2 * l + c).start()

    for copy in small:
        copy.wait()
    idr = ids[...]
    lane_e = lax.broadcasted_iota(jnp.int32, (ep, t_rows), 0)
    first, second = lane_e == idr[0:1], lane_e == idr[1:2]
    mask = jnp.where(first | second, 1.0, 0.0)
    before = jnp.where(
        lax.broadcasted_iota(jnp.int32, (t_rows, t_rows), 0)
        < lax.broadcasted_iota(jnp.int32, (t_rows, t_rows), 1), 1.0, 0.0).astype(BF16)
    rank = jnp.dot(mask.astype(BF16), before, preferred_element_type=F32)
    key = jnp.where(mask > 0.0, rank, -1.0)
    slot = lax.broadcasted_iota(jnp.int32, (cap, t_rows), 0).astype(F32)
    for x in range(ep):
        hot[x * cap:(x + 1) * cap] = jnp.where(key[x:x + 1] == slot, 1.0, 0.0).astype(BF16)

    def select(a):
        stage[a] = jnp.dot(
            hot[...], xin[a, :, col(j)], preferred_element_type=F32).astype(BF16)

    loads[0].wait()
    select(0)
    pl.semaphore_wait(barrier, ep + tp - 2)
    if far:
        send(core, (0,))
    loads[1].wait()
    select(1)
    if far:
        send(core, (1,))

    p = probs[...].astype(F32)
    chosen = (jnp.where(first, p[0:1], 0.0) + jnp.where(second, p[1:2], 0.0)).astype(BF16)
    slot_p = lax.dot_general(chosen, hot[...], NT, preferred_element_type=F32)
    for x in range(ep):
        pw_out[x, :, :cap] = slot_p[x:x + 1, x * cap:(x + 1) * cap]

    def w_start(n, _):
        w_copy(lax.rem(e + n, ep), e).start()
        return 0

    lax.fori_loop(1, ep, w_start, 0)
    pw_in[e] = pw_out[e]

    for a in range(2):
        for n in range(width // tile):
            cs = pl.ds(n * tile, tile)
            mate_rows[a, :, cs] = jnp.dot(
                hot[blk(mate)], xin[a, :, cs], preferred_element_type=F32).astype(BF16)
        m_copy(a, e).start()
    for a in range(2):
        for n in range(width // tile):
            cs = pl.ds(n * tile, tile)
            rows[a, blk(e), cs] = jnp.dot(
                hot[blk(e)], xin[a, :, cs], preferred_element_type=F32).astype(BF16)
    for n in range(2, 5):
        loads[n].wait()

    def arrive(u):
        s = source(u + 2)
        for a in range(2):
            z_wait(a, s).wait_recv()
            for copy in gather_step(a, s, 0, False):
                copy.start()

    def spread(u, n):
        s = source(u + 2)
        for a in range(2):
            for copy in gather_step(a, s, n - 1, True):
                copy.wait_recv()
            for copy in gather_step(a, s, n, False):
                copy.start()

    def feed(u):
        @pl.when(core == u % 2)
        def _():
            send(u, (0, 1))

    def feed_whole():
        near = 2 * level_of(far - 1)
        for a in range(2):
            for c in range(2):
                for n in range(width // tile):
                    cs = pl.ds(n * tile, tile)
                    whole[a, c, :, cs] = jnp.dot(
                        hot[blk(near + c)], xin[a, :, cs], preferred_element_type=F32).astype(BF16)
                full_copy(a, c, e, near + c).start()

    def compute(v):
        s = source(v)
        @pl.when(v == 1)
        def _():
            for a in range(2):
                m_copy(a, mate).wait_recv()
        if far:
            @pl.when(v == units - 1)
            def _():
                for a in range(2):
                    full_copy(a, 0, s, s).wait_recv()
        @pl.when(jnp.logical_and(v >= 2, v < units - 1))
        def _():
            for a in range(2):
                for copy in gather_step(a, s, nb - 1, True):
                    copy.wait_recv()
        @pl.when(v >= 1)
        def _():
            w_copy(s, s).wait_recv()
        x = rows[0, blk(s), :]
        pre_gate = lax.dot_general(x, weights[0], NT, preferred_element_type=F32)
        pre_up = lax.dot_general(x, weights[1], NT, preferred_element_type=F32)
        back = lax.dot_general(rows[1, blk(s), :], weights[2], NT, preferred_element_type=F32)
        p = jnp.broadcast_to(pw_in[s], (8, t_rows)).T[:cap, 0:1]
        sigma = jax.nn.sigmoid(pre_gate)
        silu = pre_gate * sigma
        hidden = silu * pre_up
        scaled = p * back
        gg = (scaled * pre_up * sigma * (1.0 + pre_gate * (1.0 - sigma))).astype(BF16)
        gu = (scaled * silu).astype(BF16)
        for n in range(width // tile):
            cs = pl.ds(n * tile, tile)
            part[s, :, cs] = (
                jnp.dot(gg, weights[0, :, cs], preferred_element_type=F32)
                + jnp.dot(gu, weights[1, :, cs], preferred_element_type=F32)).astype(BF16)
        for copy, _, _ in scatter_step(s, 0, False):
            copy.start()
        grads[0, blk(s)] = gg
        grads[1, blk(s)] = gu
        grads[2, blk(s)] = (p * hidden).astype(BF16)
        prod = jnp.sum(hidden * back, axis=1, keepdims=True)
        r_send[s, :, :cap] = jnp.broadcast_to(prod, (cap, t_rows)).T[0:1]
        @pl.when(v >= 1)
        def _():
            r_copy(s, e).start()
        @pl.when(v == 0)
        def _():
            r_in[e] = r_send[e]

    def merge(v, n):
        s = source(v)
        for (copy, _, _), (_, mine, got) in zip(scatter_step(s, n, False), scatter_step(s, n, True)):
            copy.wait()
            mine[...] = (mine[...].astype(F32) + got[...].astype(F32)).astype(BF16)
        if n + 1 < nb:
            for copy, _, _ in scatter_step(s, n + 1, False):
                copy.start()
        else:
            @pl.when(v >= 1)
            def _():
                pz_copy(s, e).start()
            @pl.when(v == 0)
            def _():
                z_in[blk(e)] = part[e, :, col(j)]

    outs = (gate_out, up_out, down_out)

    def weight_grad(k):
        left = grads[k].T
        for n in range(width // tile):
            cs = pl.ds(n * tile, tile)
            outs[k][:, cs] = jnp.dot(left, rows[k // 2, :, cs], preferred_element_type=F32)

    begin = nb + AHEAD + 1
    last = units - 2 + begin

    def tick(t, _):
        def stage_of(f, i, low, high):
            @pl.when(jnp.logical_and(i >= low, i < high))
            def _():
                f(i)

        stage_of(compute, jnp.where(t < 2, t, jnp.where(t >= begin, t - begin + 2, -1)), 0, units)
        if far:
            stage_of(feed, jnp.where(t == 1, 2, jnp.where(t > 2, t, 0)), 2, far - 1)
            @pl.when(jnp.logical_and(t == max(1, far - 3), core == 1))
            def _():
                feed_whole()
            stage_of(arrive, t - 1, 0, far - 1)
            for n in range(1, nb):
                stage_of(functools.partial(spread, n=n), t - 1 - n, 0, far - 1)
        @pl.when(t == last)
        def _():
            weight_grad(0)
        @pl.when(t == last + 1)
        def _():
            lax.fori_loop(1, ep, r_wait, 0)
            lax.fori_loop(1, tp, rt_start, 0)
            r_tp[j] = r_in[...]
            weight_grad(1)
        for n in range(nb - 1, -1, -1):
            own, other = t - 1 - n, t - begin - 1 - n + 2
            stage_of(functools.partial(merge, n=n), jnp.where(
                own < 2, own, jnp.where(other >= 2, other, -1)), 0, units)
        return 0

    def r_wait(n, _):
        s = lax.rem(e + n, ep)
        r_copy(s, s).wait()
        return 0

    def rt_copy(d, s):
        return remote(r_in, r_tp.at[s], rt_send.at[d], rt_recv.at[s], e, d)

    def rt_start(n, _):
        rt_copy(lax.rem(j + n, tp), j).start()
        return 0

    def rt_wait(n, _):
        s = lax.rem(j + n, tp)
        rt_copy(s, s).wait()
        return 0

    lax.fori_loop(0, last + nb + 1, tick, 0)
    weight_grad(2)
    hot_t[...] = hot[...].T
    lax.fori_loop(1, tp, rt_wait, 0)
    for x in range(ep):
        total = r_tp[0, x]
        for i in range(1, tp):
            total = total + r_tp[i, x]
        r_mat[x:x + 1, :cap] = total[:, :cap]
    sums = r_mat[...].T
    found = [jnp.zeros((1, t_rows), F32) for _ in range(2)]
    for x in range(ep):
        value = jnp.sum(
            hot[x * cap:(x + 1) * cap].astype(F32) * sums[:cap, x:x + 1], axis=0, keepdims=True)
        found = [f + jnp.where(idr[k:k + 1] == x, value, 0.0) for k, f in enumerate(found)]
    for k in range(2):
        route_out[k:k + 1] = found[k]

    def pz_wait(n, _):
        s = lax.rem(e + n, ep)
        pz_copy(s, s).wait()
        return 0

    lax.fori_loop(1, ep, pz_wait, 0)
    dx_out[...] = jnp.dot(hot_t[...], z_in[...], preferred_element_type=F32).astype(BF16)
    def finish(n, _):
        d = lax.rem(e + n, ep)
        w_copy(d, e).wait_send()
        if far:
            @pl.when(jnp.logical_and(d // 2 != lvl, jnp.logical_or(core == 0, d // 2 != level_of(far - 1))))
            def _():
                for a in range(2):
                    z_copy(a, d).wait_send()
            @pl.when(jnp.logical_and(d // 2 != lvl, d != 2 * level_of(far - 1) + 1))
            def _():
                for a in range(2):
                    for i in range(nb):
                        for copy in gather_step(a, d, i, False):
                            copy.wait_send()
        return 0

    if far:
        @pl.when(core == 1)
        def _():
            for a in range(2):
                for c in range(2):
                    full_copy(a, c, e, 2 * level_of(far - 1) + c).wait_send()
    lax.fori_loop(1, ep, finish, 0)
    for a in range(2):
        m_copy(a, e).wait_send()


def publish(*refs):
    srcs, dsts, sem = refs[:5], refs[5:10], refs[10]
    copies = [pltpu.make_async_copy(srcs[k], dsts[k], sem.at[k]) for k in (2, 3, 4, 0, 1)]
    for copy in copies:
        copy.start()
    for copy in copies:
        copy.wait()


def per_device(tokens, cotangent, expert_ids, route_weight, gate_weight, up_weight, down_weight):
    ep, tp = lax.axis_size("ep"), lax.axis_size("tp")
    t_rows, width = tokens.shape
    top = expert_ids.shape[1]
    _, f_rows, _ = gate_weight.shape
    cap = min(t_rows, 2 * top * t_rows // ep)
    span = width // tp
    nb = tp.bit_length() - 1
    any_, vmem = pl.BlockSpec(memory_space=pl.ANY), pl.BlockSpec(memory_space=pltpu.VMEM)
    dma = pltpu.SemaphoreType.DMA
    big = pltpu.VMEM((f_rows, width), F32)
    scratch = [
        pltpu.VMEM(expert_ids.shape[::-1], jnp.int32),
        pltpu.VMEM(route_weight.shape[::-1], route_weight.dtype),
        pltpu.VMEM((2, t_rows, width), BF16),
        pltpu.VMEM((ep * cap, t_rows), BF16),
        pltpu.VMEM((t_rows, ep * cap), BF16),
        pltpu.VMEM((2, ep * cap, span), BF16),
        pltpu.VMEM((2, cap, width), BF16),
        pltpu.VMEM((2, 2, cap, width), BF16),
        pltpu.VMEM((2, ep * cap, width), BF16),
        pltpu.VMEM((3, f_rows, width), BF16),
        pltpu.VMEM((ep, 1, t_rows), F32),
        pltpu.VMEM((ep, 1, t_rows), F32),
        pltpu.VMEM((3, ep * cap, f_rows), BF16),
        pltpu.VMEM((ep, cap, width), BF16),
        pltpu.VMEM((ep, cap // 2, (tp - 1) * span), BF16),
        pltpu.VMEM((ep, tp - 1, cap // 2, span), BF16),
        pltpu.VMEM((ep * cap, span), BF16),
        pltpu.VMEM((ep, 1, t_rows), F32),
        pltpu.VMEM((ep, 1, t_rows), F32),
        pltpu.VMEM((tp, ep, 1, t_rows), F32),
        pltpu.VMEM((ep, t_rows), F32),
        dma((7,)), dma((2, ep)), dma((2, ep)), dma((2,)), dma((2,)), dma((2, 2)), dma((2,)), dma((ep,)), dma((ep,)),
        dma((ep, nb)), dma((ep, nb)), dma((ep, tp - 1)), dma((ep, tp - 1)),
        dma((ep, nb)), dma((ep, nb)), dma((ep, tp - 1)), dma((ep, tp - 1)),
        dma((ep,)), dma((ep,)), dma((ep,)), dma((ep,)), dma((tp,)), dma((tp,)),
    ]
    pieces = pl.pallas_call(
        functools.partial(kernel, ep, tp, cap),
        out_shape=(
            pltpu.VMEM((t_rows, span), BF16),
            pltpu.VMEM(expert_ids.shape[::-1], F32), big, big, big),
        in_specs=[any_] * 7,
        out_specs=(vmem,) * 5,
        scratch_shapes=scratch,
        compiler_params=pltpu.CompilerParams(
            collective_id=0, has_side_effects=True,
            vmem_limit_bytes=VMEM_BYTES - 12 * f_rows * width - 2 * t_rows * span),
    )(tokens, cotangent, expert_ids.T, route_weight.T, gate_weight[0], up_weight[0], down_weight[0])
    dx, route, *wide = pl.pallas_call(
        publish,
        out_shape=tuple(jax.ShapeDtypeStruct(v.shape, v.dtype) for v in pieces),
        in_specs=[vmem] * 5,
        out_specs=(any_,) * 5,
        scratch_shapes=[dma((5,))],
        compiler_params=pltpu.CompilerParams(vmem_limit_bytes=1_000_000),
    )(*(pltpu.with_memory_space_constraint(v, pltpu.VMEM) for v in pieces))
    return dx, route.T, *(g[None] for g in wide)


def solution(mesh):
    in_specs = (
        P("ep", None), P("ep", None), P("ep", None), P("ep", None),
        P("ep", "tp", None), P("ep", "tp", None), P("ep", "tp", None),
    )
    out_specs = (
        P("ep", "tp"), P("ep", None), P("ep", "tp", None), P("ep", "tp", None), P("ep", "tp", None),
    )
    return jax.shard_map(
        per_device, mesh=mesh, in_specs=in_specs, out_specs=out_specs, check_vma=False
    )
```

```python
import functools

import jax
import jax.numpy as jnp
from jax import lax
from jax.experimental import pallas as pl
from jax.experimental.pallas import tpu as pltpu
from jax.sharding import PartitionSpec as P

MESH = pl.DeviceIdType.MESH
F32 = jnp.float32
BF16 = jnp.bfloat16
NT = (((1,), (1,)), ((), ()))
TN = (((0,), (0,)), ((), ()))
VMEM_BYTES = 66_900_000


def slices_for(j, bits, count):
    base = j
    for bit in bits:
        base = base - ((j // bit) % 2) * bit
    out = []
    for k in range(count):
        out.append(base + sum(bit for n, bit in enumerate(bits) if (k >> n) & 1))
    return out


def kernel(
    ep, tp, cap, tokens, cotangent, ids_in, probs_in, gate_w, up_w, down_w,
    dx_out, route_out, gate_out, up_out, down_out,
    ids, probs, xin, hot, hot_t, stage, mate_rows, whole, diag, rows, weights, pw_out, pw_in, grads, part, ta_in, tb_in, z_in,
    r_send, r_in, r_tp, r_mat,
    load_sem, z_send, z_recv, m_send, m_recv, f_send, f_recv, x_send, x_recv, d_send, d_recv,
    w_send, w_recv, t_send, t_recv, p_send, p_recv, pz_send, pz_recv, rs_send, rs_recv,
    rt_send, rt_recv,
):
    e, j = lax.axis_index("ep"), lax.axis_index("tp")
    levels = ep // 2
    lvl, core = e // 2, e % 2
    mate = e + 1 - 2 * core
    t_rows, width = tokens.shape
    span = width // tp
    half = cap // 2
    nb = tp.bit_length() - 1
    lb = levels.bit_length() - 1
    far = 2 * (levels - 1)
    units = far + 2
    crossed = False
    first_spread = 1 if crossed else 0
    spread_end = far - 1
    spreads = spread_end - first_spread
    tile = min(width, 512)

    def xor(a, b):
        out = 0
        for n in range(lb):
            p, q = (a // (1 << n)) % 2, (b // (1 << n)) % 2
            out = out + (p + q - 2 * p * q) * (1 << n)
        return out

    def level_of(u):
        d = u // 2 + 1 + u % 2
        return xor(lvl, jnp.where(d >= levels, 1, d))

    def source(w):
        v = jnp.where(w == units - 2, units - 1, jnp.where(w == units - 1, units - 2, w)) if far else w
        u = jnp.maximum(v - 2, 0)
        return jnp.where(v == 0, e, jnp.where(v == 1, mate, 2 * level_of(u) + u % 2))

    def blk(s):
        return pl.ds(pl.multiple_of(s * cap, cap), cap)

    def col(s):
        return pl.ds(pl.multiple_of(s * span, span), span)

    def run(first, count):
        return pl.ds(pl.multiple_of(first * span, span), count * span)

    def flip(bit):
        return j + bit * (1 - 2 * ((j // bit) % 2))

    def remote(src, dst, ssem, rsem, de, dt):
        return pltpu.make_async_remote_copy(
            src_ref=src, dst_ref=dst, send_sem=ssem, recv_sem=rsem,
            device_id=(de, dt), device_id_type=MESH)

    small = [
        pltpu.make_async_copy(ids_in, ids, load_sem.at[5]),
        pltpu.make_async_copy(probs_in, probs, load_sem.at[6]),
    ]
    loads = [
        pltpu.make_async_copy(tokens, xin.at[0], load_sem.at[0]),
        pltpu.make_async_copy(cotangent, xin.at[1], load_sem.at[1]),
        pltpu.make_async_copy(gate_w, weights.at[0], load_sem.at[2]),
        pltpu.make_async_copy(up_w, weights.at[1], load_sem.at[3]),
        pltpu.make_async_copy(down_w, weights.at[2], load_sem.at[4]),
    ]
    for copy in small + loads:
        copy.start()
    barrier = pltpu.get_barrier_semaphore()

    def greet(n, _):
        pl.semaphore_signal(barrier, inc=1, device_id=(lax.rem(e + n, ep), j), device_id_type=MESH)
        return 0

    def greet_tp(n, _):
        pl.semaphore_signal(barrier, inc=1, device_id=(e, lax.rem(j + n, tp)), device_id_type=MESH)
        return 0

    lax.fori_loop(1, ep, greet, 0)
    lax.fori_loop(1, tp, greet_tp, 0)

    def z_copy(a, u, d):
        return remote(stage.at[a, blk(d)], rows.at[a, blk(e), col(j)],
                      z_send, z_recv.at[a, u], d, j)

    def z_wait(a, u, s):
        return remote(stage.at[a, blk(s)], rows.at[a, blk(s), col(j)],
                      z_send, z_recv.at[a, u], s, j)

    def m_copy(s):
        return remote(mate_rows, rows.at[:, blk(s)], m_send, m_recv, mate, j)

    def full_copy(c, s, d):
        return remote(whole.at[c], rows.at[:, blk(s)], f_send, f_recv, d, j)

    def cross_copy(bit, s, receive):
        peer = flip(bit)
        ref = rows.at[:, blk(s), col(peer if receive else j)]
        return remote(ref, ref, x_send, x_recv.at[bit - 1], e, peer)

    def diag_copy(c, s, d):
        return remote(diag.at[c], rows.at[:, blk(s), col(tp - 1 - j)], d_send, d_recv, d, j)

    def w_copy(d, s):
        return remote(pw_out.at[d], pw_in.at[s], w_send, w_recv.at[0], d, j)

    def w_mate(s):
        return remote(pw_out.at[mate], pw_in.at[s], w_send, w_recv.at[1], mate, j)

    def gather_step(a, u, s, n):
        peer = flip(1 << n if a == 0 else tp >> (n + 1))
        if a == 0:
            ref = rows.at[a, blk(s), run(j - j % (1 << n), 1 << n)]
            return [remote(ref, ref, t_send, t_recv.at[a, u, n], e, peer)]
        copies = []
        for sid in slices_for(j, [tp >> (i + 1) for i in range(n)], 1 << n):
            ref = rows.at[a, blk(s), col(sid)]
            copies.append(remote(ref, ref, t_send, t_recv.at[a, u, n], e, peer))
        return copies

    def gather_wait(a, u, s, n):
        ref = rows.at[a, blk(s), run(0, 1 << n)]
        remote(ref, ref, t_send, t_recv.at[a, u, n], e, flip(1)).wait_recv()

    def scatter_step(w, s, n):
        base, count = tp - (tp >> n), tp >> (n + 1)
        copies = []
        for k in range(count):
            peer = flip(1 << n)
            bits = [1 << i for i in range(n + 1, nb)]
            mine = part.at[s, :half, col(slices_for(j, bits, count)[k])]
            src = part.at[s, :half, col(slices_for(peer, bits, count)[k])]
            got = tb_in.at[s, base + k]
            copies.append((remote(src, got, p_send, p_recv.at[w, n], e, peer), mine, got))
        peer = flip(count)
        mine = part.at[s, half:, run(j - j % count, count)]
        src = part.at[s, half:, run(peer - peer % count, count)]
        got = ta_in.at[s, :, base * span:(base + count) * span]
        copies.append((remote(src, got, p_send, p_recv.at[w, n], e, peer), mine, got))
        return copies

    def scatter_wait(w, n):
        ref = part.at[0, :, run(0, tp >> (n + 1))]
        remote(ref, ref, p_send, p_recv.at[w, n], e, flip(1)).wait_recv()

    def pz_copy(d, s):
        return remote(part.at[d, :, col(j)], z_in.at[blk(s)], pz_send, pz_recv, d, j)

    def r_copy(d, s):
        return remote(r_send.at[d], r_in.at[s], rs_send, rs_recv, d, j)

    def send(u, arrays):
        l = level_of(u)
        for a in arrays:
            for c in range(2):
                z_copy(a, u, 2 * l + c).start()

    for copy in small:
        copy.wait()
    idr = ids[...]
    lane_e = lax.broadcasted_iota(jnp.int32, (ep, t_rows), 0)
    first, second = lane_e == idr[0:1], lane_e == idr[1:2]
    mask = jnp.where(first | second, 1.0, 0.0)
    before = jnp.where(
        lax.broadcasted_iota(jnp.int32, (t_rows, t_rows), 0)
        < lax.broadcasted_iota(jnp.int32, (t_rows, t_rows), 1), 1.0, 0.0).astype(BF16)
    rank = jnp.dot(mask.astype(BF16), before, preferred_element_type=F32)
    key = jnp.where(mask > 0.0, rank, -1.0)
    slot = lax.broadcasted_iota(jnp.int32, (cap, t_rows), 0).astype(F32)
    for x in range(ep):
        hot[x * cap:(x + 1) * cap] = jnp.where(key[x:x + 1] == slot, 1.0, 0.0).astype(BF16)

    def select(a):
        stage[a] = jnp.dot(
            hot[...], xin[a, :, col(j)], preferred_element_type=F32).astype(BF16)

    for a in range(2):
        loads[a].wait()
        select(a)
        for n in range(width // tile):
            cs = pl.ds(n * tile, tile)
            mate_rows[a, :, cs] = jnp.dot(
                hot[blk(mate)], xin[a, :, cs], preferred_element_type=F32).astype(BF16)
            rows[a, blk(e), cs] = jnp.dot(
                hot[blk(e)], xin[a, :, cs], preferred_element_type=F32).astype(BF16)

    p = probs[...].astype(F32)
    chosen = (jnp.where(first, p[0:1], 0.0) + jnp.where(second, p[1:2], 0.0)).astype(BF16)
    slot_p = lax.dot_general(chosen, hot[...], NT, preferred_element_type=F32)
    for x in range(ep):
        pw_out[x, :, :cap] = slot_p[x:x + 1, x * cap:(x + 1) * cap]
    pw_in[e] = pw_out[e]

    def w_start(n, _):
        d = lax.rem(e + n, ep)
        @pl.when(d != mate)
        def _():
            w_copy(d, e).start()
        return 0

    pl.semaphore_wait(barrier, ep + tp - 2)
    lax.fori_loop(1, ep, w_start, 0)
    w_mate(e).start()
    if far:
        send(core, (0, 1))
    m_copy(e).start()
    if crossed:
        @pl.when(core == 0)
        def _():
            for a in range(2):
                for c in range(2):
                    diag[c, a] = jnp.dot(
                        hot[blk(2 * level_of(0) + c)], xin[a, :, col(tp - 1 - j)],
                        preferred_element_type=F32).astype(BF16)
            for c in range(2):
                diag_copy(c, e, 2 * level_of(0) + c).start()
    for n in range(2, 5):
        loads[n].wait()

    def source_of(u):
        return 2 * level_of(u) + u % 2

    def arrive(u):
        s = source_of(u)
        for a in range(2):
            z_wait(a, u, s).wait_recv()
            @pl.when(u >= first_spread)
            def _():
                for copy in gather_step(a, u, s, 0):
                    copy.start()
        if crossed:
            @pl.when(u == 0)
            def _():
                for bit in (1, 2):
                    cross_copy(bit, s, False).start()

    def spread(u, n):
        s = source_of(u)
        for a in range(2):
            gather_wait(a, u, s, n - 1)
            for copy in gather_step(a, u, s, n):
                copy.start()

    def feed(u):
        @pl.when(core == u % 2)
        def _():
            send(u, (0, 1))

    def feed_whole():
        near = 2 * level_of(far - 1)
        for c in range(2):
            for a in range(2):
                for n in range(width // tile):
                    cs = pl.ds(n * tile, tile)
                    whole[c, a, :, cs] = jnp.dot(
                        hot[blk(near + c)], xin[a, :, cs], preferred_element_type=F32).astype(BF16)
            full_copy(c, e, near + c).start()

    def compute(w):
        s = source(w)
        @pl.when(w == 1)
        def _():
            m_copy(mate).wait_recv()
            w_mate(mate).wait_recv()
        if far:
            @pl.when(w == 2)
            def _():
                some = pw_in.at[pl.ds(0, ep - 2)]
                remote(some, some, w_send, w_recv.at[0], mate, j).wait_recv()
            if crossed:
                @pl.when(w == 2)
                def _():
                    for bit in (1, 2):
                        cross_copy(bit, s, True).wait_recv()
                    diag_copy(0, s, s).wait_recv()
            @pl.when(w == units - 2)
            def _():
                full_copy(0, s, s).wait_recv()
            u = jnp.where(w == units - 1, spread_end - 1, w - 2)
            @pl.when(jnp.logical_and(w != units - 2, w >= 2 + first_spread))
            def _():
                for a in range(2):
                    gather_wait(a, u, s, nb - 1)
        x = rows[0, blk(s), :]
        pre_gate = lax.dot_general(x, weights[0], NT, preferred_element_type=F32)
        pre_up = lax.dot_general(x, weights[1], NT, preferred_element_type=F32)
        back = lax.dot_general(rows[1, blk(s), :], weights[2], NT, preferred_element_type=F32)
        p = jnp.broadcast_to(pw_in[s], (8, t_rows)).T[:cap, 0:1]
        sigma = jax.nn.sigmoid(pre_gate)
        silu = pre_gate * sigma
        hidden = silu * pre_up
        scaled = p * back
        gg = (scaled * pre_up * sigma * (1.0 + pre_gate * (1.0 - sigma))).astype(BF16)
        gu = (scaled * silu).astype(BF16)
        for n in range(width // tile):
            cs = pl.ds(n * tile, tile)
            part[s, :, cs] = (
                jnp.dot(gg, weights[0, :, cs], preferred_element_type=F32)
                + jnp.dot(gu, weights[1, :, cs], preferred_element_type=F32)).astype(BF16)
        for copy, _, _ in scatter_step(w, s, 0):
            copy.start()
        grads[0, blk(s)] = gg
        grads[1, blk(s)] = gu
        grads[2, blk(s)] = (p * hidden).astype(BF16)
        prod = jnp.sum(hidden * back, axis=1, keepdims=True)
        r_send[s, :, :cap] = jnp.broadcast_to(prod, (cap, t_rows)).T[0:1]
        @pl.when(w >= 1)
        def _():
            r_copy(s, e).start()
        @pl.when(w == 0)
        def _():
            r_in[e] = r_send[e]

    def merge(w, n):
        s = source(w)
        scatter_wait(w, n)
        for _, mine, got in scatter_step(w, s, n):
            mine[...] = (mine[...].astype(F32) + got[...].astype(F32)).astype(BF16)
        if n + 1 < nb:
            for copy, _, _ in scatter_step(w, s, n + 1):
                copy.start()
        else:
            @pl.when(w >= 1)
            def _():
                pz_copy(s, e).start()
            @pl.when(w == 0)
            def _():
                z_in[blk(e)] = part[e, :, col(j)]

    outs = (gate_out, up_out, down_out)

    def weight_grad(k):
        left = grads[k].T
        for n in range(width // tile):
            cs = pl.ds(n * tile, tile)
            outs[k][:, cs] = jnp.dot(left, rows[k // 2, :, cs], preferred_element_type=F32)

    def rt_copy(d, s):
        return remote(r_in, r_tp.at[s], rt_send, rt_recv, e, d)

    def rt_start(n, _):
        rt_copy(lax.rem(j + n, tp), j).start()
        return 0

    final = units + nb - 2

    bulk = units + nb - 3

    def done(t):
        count = jnp.where(t > bulk, units, jnp.clip(t - nb, 2, units))
        return jnp.where(t < 2, jnp.maximum(t, 0), count)

    def span_of(f, low, high):
        def one(w, _):
            f(w)
            return 0

        lax.fori_loop(low, high, one, 0)

    def merges(t, when):
        @pl.when(when)
        def _():
            for n in range(nb - 1, -1, -1):
                late = functools.partial(merge, n=n)
                if n == 0:
                    span_of(late, done(t - 1), done(t))
                else:
                    span_of(late, jnp.minimum(done(t - 2 - n), 2), jnp.minimum(done(t - 1 - n), 2))
                    span_of(late, jnp.maximum(done(t - 1 - n), 2), jnp.maximum(done(t - n), 2))
            @pl.when(t == final)
            def _():
                lines = r_in.at[pl.ds(0, ep - 1)]
                remote(lines, lines, rs_send, rs_recv, mate, j).wait()
                lax.fori_loop(1, tp, rt_start, 0)
                r_tp[j] = r_in[...]
                for k in range(0):
                    weight_grad(k)

    def tick(t, _):
        def stage_of(f, i, low, high):
            @pl.when(jnp.logical_and(i >= low, i < high))
            def _():
                f(i)

        if far:
            stage_of(feed, jnp.where(t > 2, t, 0), 2, far - 1)
            @pl.when(jnp.logical_and(t == max(1, far - 3), core == 1))
            def _():
                feed_whole()
        merges(t, t >= bulk - 1)
        span_of(compute, done(t), done(t + 1))
        if far:
            stage_of(feed, jnp.where(t == 1, 2, 0), 2, far - 1)
            stage_of(arrive, jnp.where(t <= 2, t - 1, -1), 0, far - 1)
        merges(t, t < bulk - 1)
        if far:
            for n in range(1, nb):
                stage_of(functools.partial(spread, n=n), t - 1 - n, first_spread, spread_end)
            stage_of(arrive, jnp.where(t > 2, t - 1, -1), 0, far - 1)
        return 0

    lax.fori_loop(0, units + 2 * nb - 2, tick, 0)
    for k in range(0, 3):
        weight_grad(k)
    hot_t[...] = hot[...].T
    lines = r_tp.at[pl.ds(0, tp - 1)]
    remote(lines, lines, rt_send, rt_recv, e, flip(1)).wait()
    for x in range(ep):
        total = r_tp[0, x]
        for i in range(1, tp):
            total = total + r_tp[i, x]
        r_mat[x:x + 1, :cap] = total[:, :cap]
    sums = r_mat[...].T
    found = [jnp.zeros((1, t_rows), F32) for _ in range(2)]
    for x in range(ep):
        value = jnp.sum(
            hot[x * cap:(x + 1) * cap].astype(F32) * sums[:cap, x:x + 1], axis=0, keepdims=True)
        found = [f + jnp.where(idr[k:k + 1] == x, value, 0.0) for k, f in enumerate(found)]
    for k in range(2):
        route_out[k:k + 1] = found[k]

    lines = pw_out.at[pl.ds(0, ep - 1)]
    remote(lines, lines, w_send, w_recv.at[0], mate, j).wait_send()
    m_copy(e).wait_send()
    if far:
        @pl.when(core == 0)
        def _():
            sent = stage.at[:, :far * cap]
            remote(sent, sent, z_send, z_recv.at[0, 0], mate, j).wait_send()
            if crossed:
                remote(diag, diag, d_send, d_recv, mate, j).wait_send()
        @pl.when(core == 1)
        def _():
            if far > 2:
                sent = stage.at[:, :(far - 2) * cap]
                remote(sent, sent, z_send, z_recv.at[0, 0], mate, j).wait_send()
            remote(whole, whole, f_send, f_recv, mate, j).wait_send()
        if crossed:
            sent = rows.at[:, :cap, :2 * span]
            remote(sent, sent, x_send, x_recv.at[0], e, flip(1)).wait_send()
        if spreads:
            sent = rows.at[:, :spreads * cap, :(tp - 1) * span]
            remote(sent, sent, t_send, t_recv.at[0, 0, 0], e, flip(1)).wait_send()
    sent = part.at[:, :, :(tp - 1) * span]
    remote(sent, sent, p_send, p_recv.at[0, 0], e, flip(1)).wait_send()
    sent = z_in.at[:(ep - 1) * cap]
    remote(sent, sent, pz_send, pz_recv, mate, j).wait()
    dx_out[...] = jnp.dot(hot_t[...], z_in[...], preferred_element_type=F32).astype(BF16)


def publish(*refs):
    srcs, dsts, sem = refs[:5], refs[5:10], refs[10]
    copies = [pltpu.make_async_copy(srcs[k], dsts[k], sem.at[k]) for k in (2, 3, 4, 0, 1)]
    for copy in copies:
        copy.start()
    for copy in copies:
        copy.wait()


def per_device(tokens, cotangent, expert_ids, route_weight, gate_weight, up_weight, down_weight):
    ep, tp = lax.axis_size("ep"), lax.axis_size("tp")
    t_rows, width = tokens.shape
    top = expert_ids.shape[1]
    _, f_rows, _ = gate_weight.shape
    cap = min(t_rows, 2 * top * t_rows // ep)
    span = width // tp
    nb = tp.bit_length() - 1
    any_, vmem = pl.BlockSpec(memory_space=pl.ANY), pl.BlockSpec(memory_space=pltpu.VMEM)
    dma = pltpu.SemaphoreType.DMA
    big = pltpu.VMEM((f_rows, width), F32)
    scratch = [
        pltpu.VMEM(expert_ids.shape[::-1], jnp.int32),
        pltpu.VMEM(route_weight.shape[::-1], route_weight.dtype),
        pltpu.VMEM((2, t_rows, width), BF16),
        pltpu.VMEM((ep * cap, t_rows), BF16),
        pltpu.VMEM((t_rows, ep * cap), BF16),
        pltpu.VMEM((2, ep * cap, span), BF16),
        pltpu.VMEM((2, cap, width), BF16),
        pltpu.VMEM((2, 2, cap, width), BF16),
        pltpu.VMEM((2, 2, cap, span), BF16),
        pltpu.VMEM((2, ep * cap, width), BF16),
        pltpu.VMEM((3, f_rows, width), BF16),
        pltpu.VMEM((ep, 1, t_rows), F32),
        pltpu.VMEM((ep, 1, t_rows), F32),
        pltpu.VMEM((3, ep * cap, f_rows), BF16),
        pltpu.VMEM((ep, cap, width), BF16),
        pltpu.VMEM((ep, cap // 2, (tp - 1) * span), BF16),
        pltpu.VMEM((ep, tp - 1, cap // 2, span), BF16),
        pltpu.VMEM((ep * cap, span), BF16),
        pltpu.VMEM((ep, 1, t_rows), F32),
        pltpu.VMEM((ep, 1, t_rows), F32),
        pltpu.VMEM((tp, ep, 1, t_rows), F32),
        pltpu.VMEM((ep, t_rows), F32),
        dma((7,)), dma(()), dma((2, max(ep - 3, 1))), dma(()), dma(()), dma(()), dma(()),
        dma(()), dma((2,)), dma(()), dma(()), dma(()), dma((2,)),
        dma(()), dma((2, max(ep - 3, 1), nb)), dma(()), dma((ep, nb)), dma(()), dma(()),
        dma(()), dma(()), dma(()), dma(()),
    ]
    pieces = pl.pallas_call(
        functools.partial(kernel, ep, tp, cap),
        out_shape=(
            pltpu.VMEM((t_rows, span), BF16),
            pltpu.VMEM(expert_ids.shape[::-1], F32), big, big, big),
        in_specs=[any_] * 7,
        out_specs=(vmem,) * 5,
        scratch_shapes=scratch,
        compiler_params=pltpu.CompilerParams(
            collective_id=0, has_side_effects=True,
            vmem_limit_bytes=VMEM_BYTES - 12 * f_rows * width - 2 * t_rows * span),
    )(tokens, cotangent, expert_ids.T, route_weight.T, gate_weight[0], up_weight[0], down_weight[0])
    dx, route, *wide = pl.pallas_call(
        publish,
        out_shape=tuple(jax.ShapeDtypeStruct(v.shape, v.dtype) for v in pieces),
        in_specs=[vmem] * 5,
        out_specs=(any_,) * 5,
        scratch_shapes=[dma((5,))],
        compiler_params=pltpu.CompilerParams(vmem_limit_bytes=1_000_000),
    )(*(pltpu.with_memory_space_constraint(v, pltpu.VMEM) for v in pieces))
    return dx, route.T, *(g[None] for g in wide)


def solution(mesh):
    in_specs = (
        P("ep", None), P("ep", None), P("ep", None), P("ep", None),
        P("ep", "tp", None), P("ep", "tp", None), P("ep", "tp", None),
    )
    out_specs = (
        P("ep", "tp"), P("ep", None), P("ep", "tp", None), P("ep", "tp", None), P("ep", "tp", None),
    )
    return jax.shard_map(
        per_device, mesh=mesh, in_specs=in_specs, out_specs=out_specs, check_vma=False
    )
```

```python
import functools

import jax
import jax.numpy as jnp
from jax import lax
from jax.experimental import pallas as pl
from jax.experimental.pallas import tpu as pltpu
from jax.sharding import PartitionSpec as P

MESH = pl.DeviceIdType.MESH
F32 = jnp.float32
BF16 = jnp.bfloat16
NT = (((1,), (1,)), ((), ()))
TN = (((0,), (0,)), ((), ()))
VMEM_BYTES = 66_900_000


def slices_for(j, bits, count):
    base = j
    for bit in bits:
        base = base - ((j // bit) % 2) * bit
    out = []
    for k in range(count):
        out.append(base + sum(bit for n, bit in enumerate(bits) if (k >> n) & 1))
    return out


def kernel(
    ep, tp, cap, tokens, cotangent, ids_in, probs_in, gate_w, up_w, down_w,
    dx_out, route_out, gate_out, up_out, down_out,
    ids, probs, xin, hot, hot_t, stage, mate_rows, whole, diag, rows, weights, flipped, pw_out, pw_in, grads, part, ta_in, tb_in, z_in,
    r_send, r_in, r_tp, r_mat,
    load_sem, z_send, z_recv, m_send, m_recv, f_send, f_recv, x_send, x_recv, d_send, d_recv,
    w_send, w_recv, t_send, t_recv, p_send, p_recv, pz_send, pz_recv, rs_send, rs_recv,
    rt_send, rt_recv,
):
    e, j = lax.axis_index("ep"), lax.axis_index("tp")
    levels = ep // 2
    lvl, core = e // 2, e % 2
    mate = e + 1 - 2 * core
    t_rows, width = tokens.shape
    span = width // tp
    half = cap // 2
    nb = tp.bit_length() - 1
    lb = levels.bit_length() - 1
    far = 2 * (levels - 1)
    units = far + 2
    crossed = tp == 4 and far > 2
    spread_end = far - 2 if crossed else far - 1
    tile = min(width, 512)

    def xor(a, b):
        out = 0
        for n in range(lb):
            p, q = (a // (1 << n)) % 2, (b // (1 << n)) % 2
            out = out + (p + q - 2 * p * q) * (1 << n)
        return out

    def level_of(u):
        d = u // 2 + 1 + u % 2
        return xor(lvl, jnp.where(d >= levels, 1, d))

    whole_at = units - 3 if far > 2 else units - 1

    def unit_of(w):
        return jnp.where(w == whole_at, units - 1, jnp.where(w > whole_at, w - 1, w))

    def source(w):
        v = unit_of(w)
        u = jnp.maximum(v - 2, 0)
        return jnp.where(v == 0, e, jnp.where(v == 1, mate, 2 * level_of(u) + u % 2))

    def blk(s):
        return pl.ds(pl.multiple_of(s * cap, cap), cap)

    def col(s):
        return pl.ds(pl.multiple_of(s * span, span), span)

    def run(first, count):
        return pl.ds(pl.multiple_of(first * span, span), count * span)

    def flip(bit):
        return j + bit * (1 - 2 * ((j // bit) % 2))

    def remote(src, dst, ssem, rsem, de, dt):
        return pltpu.make_async_remote_copy(
            src_ref=src, dst_ref=dst, send_sem=ssem, recv_sem=rsem,
            device_id=(de, dt), device_id_type=MESH)

    small = [
        pltpu.make_async_copy(ids_in, ids, load_sem.at[5]),
        pltpu.make_async_copy(probs_in, probs, load_sem.at[6]),
    ]
    loads = [
        pltpu.make_async_copy(tokens, xin.at[0], load_sem.at[0]),
        pltpu.make_async_copy(cotangent, xin.at[1], load_sem.at[1]),
        pltpu.make_async_copy(gate_w, weights.at[0], load_sem.at[2]),
        pltpu.make_async_copy(up_w, weights.at[1], load_sem.at[3]),
        pltpu.make_async_copy(down_w, weights.at[2], load_sem.at[4]),
    ]
    for copy in small + loads:
        copy.start()
    barrier = pltpu.get_barrier_semaphore()

    def greet(n, _):
        pl.semaphore_signal(barrier, inc=1, device_id=(lax.rem(e + n, ep), j), device_id_type=MESH)
        return 0

    def greet_tp(n, _):
        pl.semaphore_signal(barrier, inc=1, device_id=(e, lax.rem(j + n, tp)), device_id_type=MESH)
        return 0

    lax.fori_loop(1, ep, greet, 0)
    lax.fori_loop(1, tp, greet_tp, 0)

    def z_copy(a, u, d):
        return remote(stage.at[a, blk(d)], rows.at[a, blk(e), col(j)],
                      z_send, z_recv.at[a, u], d, j)

    def z_wait(a, u, s):
        return remote(stage.at[a, blk(s)], rows.at[a, blk(s), col(j)],
                      z_send, z_recv.at[a, u], s, j)

    def m_copy(s):
        return remote(mate_rows, rows.at[:, blk(s)], m_send, m_recv, mate, j)

    def full_copy(c, s, d):
        return remote(whole.at[c], rows.at[:, blk(s)], f_send, f_recv, d, j)

    def cross_copy(bit, s, receive):
        peer = flip(bit)
        ref = rows.at[:, blk(s), col(peer if receive else j)]
        return remote(ref, ref, x_send, x_recv.at[bit - 1], e, peer)

    def diag_copy(c, s, d):
        return remote(diag.at[c], rows.at[:, blk(s), col(tp - 1 - j)], d_send, d_recv, d, j)

    def w_copy(d, s):
        return remote(pw_out.at[d], pw_in.at[s], w_send, w_recv.at[0], d, j)

    def w_mate(s):
        return remote(pw_out.at[mate], pw_in.at[s], w_send, w_recv.at[1], mate, j)

    def gather_step(a, u, s, n):
        peer = flip(1 << n if a == 0 else tp >> (n + 1))
        if a == 0:
            ref = rows.at[a, blk(s), run(j - j % (1 << n), 1 << n)]
            return [remote(ref, ref, t_send, t_recv.at[a, u, n], e, peer)]
        copies = []
        for sid in slices_for(j, [tp >> (i + 1) for i in range(n)], 1 << n):
            ref = rows.at[a, blk(s), col(sid)]
            copies.append(remote(ref, ref, t_send, t_recv.at[a, u, n], e, peer))
        return copies

    def gather_wait(a, u, s, n):
        ref = rows.at[a, blk(s), run(0, 1 << n)]
        remote(ref, ref, t_send, t_recv.at[a, u, n], e, flip(1)).wait_recv()

    def scatter_step(w, s, n):
        base, count = tp - (tp >> n), tp >> (n + 1)
        copies = []
        for k in range(count):
            peer = flip(1 << n)
            bits = [1 << i for i in range(n + 1, nb)]
            mine = part.at[s, :half, col(slices_for(j, bits, count)[k])]
            src = part.at[s, :half, col(slices_for(peer, bits, count)[k])]
            got = tb_in.at[s, base + k]
            copies.append((remote(src, got, p_send, p_recv.at[w, n], e, peer), mine, got))
        peer = flip(count)
        mine = part.at[s, half:, run(j - j % count, count)]
        src = part.at[s, half:, run(peer - peer % count, count)]
        got = ta_in.at[s, :, base * span:(base + count) * span]
        copies.append((remote(src, got, p_send, p_recv.at[w, n], e, peer), mine, got))
        return copies

    def scatter_wait(w, n):
        ref = part.at[0, :, run(0, tp >> (n + 1))]
        remote(ref, ref, p_send, p_recv.at[w, n], e, flip(1)).wait_recv()

    def pz_copy(d, s):
        return remote(part.at[d, :, col(j)], z_in.at[blk(s)], pz_send, pz_recv, d, j)

    def r_copy(d, s):
        return remote(r_send.at[d], r_in.at[s], rs_send, rs_recv, d, j)

    def send(u, arrays):
        l = level_of(u)
        for a in arrays:
            for c in range(2):
                z_copy(a, u, 2 * l + c).start()

    for copy in small:
        copy.wait()
    idr = ids[...]
    lane_e = lax.broadcasted_iota(jnp.int32, (ep, t_rows), 0)
    first, second = lane_e == idr[0:1], lane_e == idr[1:2]
    mask = jnp.where(first | second, 1.0, 0.0)
    before = jnp.where(
        lax.broadcasted_iota(jnp.int32, (t_rows, t_rows), 0)
        < lax.broadcasted_iota(jnp.int32, (t_rows, t_rows), 1), 1.0, 0.0).astype(BF16)
    rank = jnp.dot(mask.astype(BF16), before, preferred_element_type=F32)
    key = jnp.where(mask > 0.0, rank, -1.0)
    slot = lax.broadcasted_iota(jnp.int32, (cap, t_rows), 0).astype(F32)
    for x in range(ep):
        hot[x * cap:(x + 1) * cap] = jnp.where(key[x:x + 1] == slot, 1.0, 0.0).astype(BF16)

    def select(a):
        stage[a] = jnp.dot(
            hot[...], xin[a, :, col(j)], preferred_element_type=F32).astype(BF16)

    for a in range(2):
        loads[a].wait()
        select(a)
        for n in range(width // tile):
            cs = pl.ds(n * tile, tile)
            mate_rows[a, :, cs] = jnp.dot(
                hot[blk(mate)], xin[a, :, cs], preferred_element_type=F32).astype(BF16)
            rows[a, blk(e), cs] = jnp.dot(
                hot[blk(e)], xin[a, :, cs], preferred_element_type=F32).astype(BF16)

    p = probs[...].astype(F32)
    chosen = (jnp.where(first, p[0:1], 0.0) + jnp.where(second, p[1:2], 0.0)).astype(BF16)
    slot_p = lax.dot_general(chosen, hot[...], NT, preferred_element_type=F32)
    for x in range(ep):
        pw_out[x, :, :cap] = slot_p[x:x + 1, x * cap:(x + 1) * cap]
    pw_in[e] = pw_out[e]

    def w_start(n, _):
        d = lax.rem(e + n, ep)
        @pl.when(d != mate)
        def _():
            w_copy(d, e).start()
        return 0

    pl.semaphore_wait(barrier, ep + tp - 2)
    lax.fori_loop(1, ep, w_start, 0)
    w_mate(e).start()
    if far:
        send(core, (0, 1))
    m_copy(e).start()

    for k in range(3):
        loads[k + 2].wait()
        for n in range(width // tile):
            cs = pl.ds(n * tile, tile)
            flipped[k, cs] = weights[k, :, cs].T

    def source_of(u):
        return 2 * level_of(u) + u % 2

    def arrive(u):
        s = source_of(u)
        for a in range(2):
            z_wait(a, u, s).wait_recv()
            @pl.when(u < spread_end)
            def _():
                for copy in gather_step(a, u, s, 0):
                    copy.start()
        if crossed:
            @pl.when(u == spread_end)
            def _():
                for bit in (1, 2):
                    cross_copy(bit, s, False).start()

    def spread(u, n):
        s = source_of(u)
        for a in range(2):
            gather_wait(a, u, s, n - 1)
            for copy in gather_step(a, u, s, n):
                copy.start()

    def feed(u):
        @pl.when(core == u % 2)
        def _():
            send(u, (0, 1))

    def feed_cross():
        there = 2 * level_of(spread_end)
        for c in range(2):
            for a in range(2):
                diag[c, a] = jnp.dot(
                    hot[blk(there + c)], xin[a, :, col(tp - 1 - j)],
                    preferred_element_type=F32).astype(BF16)
            diag_copy(c, e, there + c).start()

    def feed_whole():
        near = 2 * level_of(far - 1)
        for c in range(2):
            for a in range(2):
                for n in range(width // tile):
                    cs = pl.ds(n * tile, tile)
                    whole[c, a, :, cs] = jnp.dot(
                        hot[blk(near + c)], xin[a, :, cs], preferred_element_type=F32).astype(BF16)
            full_copy(c, e, near + c).start()

    def compute(w):
        s = source(w)
        @pl.when(w == 1)
        def _():
            m_copy(mate).wait_recv()
            w_mate(mate).wait_recv()
        if far:
            @pl.when(w == 2)
            def _():
                some = pw_in.at[pl.ds(0, ep - 2)]
                remote(some, some, w_send, w_recv.at[0], mate, j).wait_recv()
            if crossed:
                @pl.when(w == units - 1)
                def _():
                    for bit in (1, 2):
                        cross_copy(bit, s, True).wait_recv()
                    diag_copy(0, s, s).wait_recv()
            @pl.when(w == whole_at)
            def _():
                full_copy(0, s, s).wait_recv()
            u = unit_of(w) - 2
            @pl.when(jnp.logical_and(w != whole_at, jnp.logical_and(w >= 2, u < spread_end)))
            def _():
                for a in range(2):
                    gather_wait(a, u, s, nb - 1)
        x = rows[0, blk(s), :]
        pre_gate = jnp.dot(x, flipped[0], preferred_element_type=F32)
        pre_up = jnp.dot(x, flipped[1], preferred_element_type=F32)
        back = jnp.dot(rows[1, blk(s), :], flipped[2], preferred_element_type=F32)
        p = jnp.broadcast_to(pw_in[s], (8, t_rows)).T[:cap, 0:1]
        sigma = jax.nn.sigmoid(pre_gate)
        silu = pre_gate * sigma
        hidden = silu * pre_up
        scaled = p * back
        gg = (scaled * pre_up * sigma * (1.0 + pre_gate * (1.0 - sigma))).astype(BF16)
        gu = (scaled * silu).astype(BF16)
        for n in range(width // tile):
            cs = pl.ds(n * tile, tile)
            part[s, :, cs] = (
                jnp.dot(gg, weights[0, :, cs], preferred_element_type=F32)
                + jnp.dot(gu, weights[1, :, cs], preferred_element_type=F32)).astype(BF16)
        for copy, _, _ in scatter_step(w, s, 0):
            copy.start()
        grads[0, blk(s)] = gg
        grads[1, blk(s)] = gu
        grads[2, blk(s)] = (p * hidden).astype(BF16)
        prod = jnp.sum(hidden * back, axis=1, keepdims=True)
        r_send[s, :, :cap] = jnp.broadcast_to(prod, (cap, t_rows)).T[0:1]
        @pl.when(w >= 1)
        def _():
            r_copy(s, e).start()
        @pl.when(w == 0)
        def _():
            r_in[e] = r_send[e]

    def merge(w, n):
        s = source(w)
        scatter_wait(w, n)
        for _, mine, got in scatter_step(w, s, n):
            mine[...] = (mine[...].astype(F32) + got[...].astype(F32)).astype(BF16)
        if n + 1 < nb:
            for copy, _, _ in scatter_step(w, s, n + 1):
                copy.start()
        else:
            @pl.when(w >= 1)
            def _():
                pz_copy(s, e).start()
            @pl.when(w == 0)
            def _():
                z_in[blk(e)] = part[e, :, col(j)]

    outs = (gate_out, up_out, down_out)

    def weight_grad(k):
        left = grads[k].T
        for n in range(width // tile):
            cs = pl.ds(n * tile, tile)
            outs[k][:, cs] = jnp.dot(left, rows[k // 2, :, cs], preferred_element_type=F32)

    def rt_copy(d, s):
        return remote(r_in, r_tp.at[s], rt_send, rt_recv, e, d)

    def rt_start(n, _):
        rt_copy(lax.rem(j + n, tp), j).start()
        return 0


    bulk = units + nb - 3

    def done(t):
        count = jnp.where(t > bulk, units, jnp.clip(t - nb, 2, units))
        return jnp.where(t < 2, jnp.maximum(t, 0), count)

    def span_of(f, low, high):
        def one(w, _):
            f(w)
            return 0

        lax.fori_loop(low, high, one, 0)

    def merges(t, when):
        @pl.when(when)
        def _():
            for n in range(nb - 1, -1, -1):
                late = functools.partial(merge, n=n)
                if n == 0:
                    span_of(late, done(t - 1), done(t))
                else:
                    span_of(late, jnp.minimum(done(t - 2 - n), 2), jnp.minimum(done(t - 1 - n), 2))
                    span_of(late, jnp.maximum(done(t - 1 - n), 2), jnp.maximum(done(t - n), 2))

    def exchange():
        lines = r_in.at[pl.ds(0, ep - 1)]
        remote(lines, lines, rs_send, rs_recv, mate, j).wait()
        lax.fori_loop(1, tp, rt_start, 0)
        r_tp[j] = r_in[...]

    def tick(t, _):
        def stage_of(f, i, low, high):
            @pl.when(jnp.logical_and(i >= low, i < high))
            def _():
                f(i)

        if far:
            stage_of(feed, jnp.where(t > 2, t, 0), 2, far - 1)
            if crossed:
                @pl.when(jnp.logical_and(t == spread_end + 1, core == 0))
                def _():
                    feed_cross()
            @pl.when(jnp.logical_and(t == max(1, far - 3), core == 1))
            def _():
                feed_whole()
        if far > 2:
            @pl.when(t == bulk)
            def _():
                span_of(compute, whole_at, whole_at + 2)
        merges(t, t >= bulk - 1)
        span_of(compute, done(t) + jnp.where(t == bulk, 2, 0) if far > 2 else done(t), done(t + 1))
        if far:
            stage_of(feed, jnp.where(t == 1, 2, 0), 2, far - 1)
            stage_of(arrive, jnp.where(t <= 2, t - 1, -1), 0, far - 1)
        merges(t, t < bulk - 1)
        if far:
            for n in range(1, nb):
                stage_of(functools.partial(spread, n=n), t - 1 - n, 0, spread_end)
            stage_of(arrive, jnp.where(t > 2, t - 1, -1), 0, far - 1)
        return 0

    if far > 2 and nb == 2:
        lax.fori_loop(0, bulk + 1, tick, 0)
        halves, wholes = functools.partial(merge, n=0), functools.partial(merge, n=1)
        last = units - 1
        span_of(halves, last - 2, last)
        span_of(wholes, last - 3, last - 2)
        span_of(halves, last, units)
        span_of(wholes, last - 1, last)
        exchange()
        span_of(wholes, last - 2, last - 1)
        span_of(wholes, last, units)
    else:
        lax.fori_loop(0, units + 2 * nb - 2, tick, 0)
        exchange()
    for k in range(0, 3):
        weight_grad(k)
    hot_t[...] = hot[...].T
    lines = r_tp.at[pl.ds(0, tp - 1)]
    remote(lines, lines, rt_send, rt_recv, e, flip(1)).wait()
    for x in range(ep):
        total = r_tp[0, x]
        for i in range(1, tp):
            total = total + r_tp[i, x]
        r_mat[x:x + 1, :cap] = total[:, :cap]
    sums = r_mat[...].T
    found = [jnp.zeros((1, t_rows), F32) for _ in range(2)]
    for x in range(ep):
        value = jnp.sum(
            hot[x * cap:(x + 1) * cap].astype(F32) * sums[:cap, x:x + 1], axis=0, keepdims=True)
        found = [f + jnp.where(idr[k:k + 1] == x, value, 0.0) for k, f in enumerate(found)]
    for k in range(2):
        route_out[k:k + 1] = found[k]

    lines = pw_out.at[pl.ds(0, ep - 1)]
    remote(lines, lines, w_send, w_recv.at[0], mate, j).wait_send()
    m_copy(e).wait_send()
    if far:
        @pl.when(core == 0)
        def _():
            sent = stage.at[:, :far * cap]
            remote(sent, sent, z_send, z_recv.at[0, 0], mate, j).wait_send()
            if crossed:
                remote(diag, diag, d_send, d_recv, mate, j).wait_send()
        @pl.when(core == 1)
        def _():
            if far > 2:
                sent = stage.at[:, :(far - 2) * cap]
                remote(sent, sent, z_send, z_recv.at[0, 0], mate, j).wait_send()
            remote(whole, whole, f_send, f_recv, mate, j).wait_send()
        if crossed:
            sent = rows.at[:, :cap, :2 * span]
            remote(sent, sent, x_send, x_recv.at[0], e, flip(1)).wait_send()
        if spread_end:
            sent = rows.at[:, :spread_end * cap, :(tp - 1) * span]
            remote(sent, sent, t_send, t_recv.at[0, 0, 0], e, flip(1)).wait_send()
    sent = part.at[:, :, :(tp - 1) * span]
    remote(sent, sent, p_send, p_recv.at[0, 0], e, flip(1)).wait_send()
    sent = z_in.at[:(ep - 1) * cap]
    remote(sent, sent, pz_send, pz_recv, mate, j).wait()
    dx_out[...] = jnp.dot(hot_t[...], z_in[...], preferred_element_type=F32).astype(BF16)


def publish(*refs):
    srcs, dsts, sem = refs[:5], refs[5:10], refs[10]
    copies = [pltpu.make_async_copy(srcs[k], dsts[k], sem.at[k]) for k in (2, 3, 4, 0, 1)]
    for copy in copies:
        copy.start()
    for copy in copies:
        copy.wait()


def per_device(tokens, cotangent, expert_ids, route_weight, gate_weight, up_weight, down_weight):
    ep, tp = lax.axis_size("ep"), lax.axis_size("tp")
    t_rows, width = tokens.shape
    top = expert_ids.shape[1]
    _, f_rows, _ = gate_weight.shape
    cap = min(t_rows, 2 * top * t_rows // ep)
    span = width // tp
    nb = tp.bit_length() - 1
    any_, vmem = pl.BlockSpec(memory_space=pl.ANY), pl.BlockSpec(memory_space=pltpu.VMEM)
    dma = pltpu.SemaphoreType.DMA
    big = pltpu.VMEM((f_rows, width), F32)
    scratch = [
        pltpu.VMEM(expert_ids.shape[::-1], jnp.int32),
        pltpu.VMEM(route_weight.shape[::-1], route_weight.dtype),
        pltpu.VMEM((2, t_rows, width), BF16),
        pltpu.VMEM((ep * cap, t_rows), BF16),
        pltpu.VMEM((t_rows, ep * cap), BF16),
        pltpu.VMEM((2, ep * cap, span), BF16),
        pltpu.VMEM((2, cap, width), BF16),
        pltpu.VMEM((2, 2, cap, width), BF16),
        pltpu.VMEM((2, 2, cap, span), BF16),
        pltpu.VMEM((2, ep * cap, width), BF16),
        pltpu.VMEM((3, f_rows, width), BF16),
        pltpu.VMEM((3, width, f_rows), BF16),
        pltpu.VMEM((ep, 1, t_rows), F32),
        pltpu.VMEM((ep, 1, t_rows), F32),
        pltpu.VMEM((3, ep * cap, f_rows), BF16),
        pltpu.VMEM((ep, cap, width), BF16),
        pltpu.VMEM((ep, cap // 2, (tp - 1) * span), BF16),
        pltpu.VMEM((ep, tp - 1, cap // 2, span), BF16),
        pltpu.VMEM((ep * cap, span), BF16),
        pltpu.VMEM((ep, 1, t_rows), F32),
        pltpu.VMEM((ep, 1, t_rows), F32),
        pltpu.VMEM((tp, ep, 1, t_rows), F32),
        pltpu.VMEM((ep, t_rows), F32),
        dma((7,)), dma(()), dma((2, max(ep - 3, 1))), dma(()), dma(()), dma(()), dma(()),
        dma(()), dma((2,)), dma(()), dma(()), dma(()), dma((2,)),
        dma(()), dma((2, max(ep - 3, 1), nb)), dma(()), dma((ep, nb)), dma(()), dma(()),
        dma(()), dma(()), dma(()), dma(()),
    ]
    pieces = pl.pallas_call(
        functools.partial(kernel, ep, tp, cap),
        out_shape=(
            pltpu.VMEM((t_rows, span), BF16),
            pltpu.VMEM(expert_ids.shape[::-1], F32), big, big, big),
        in_specs=[any_] * 7,
        out_specs=(vmem,) * 5,
        scratch_shapes=scratch,
        compiler_params=pltpu.CompilerParams(
            collective_id=0, has_side_effects=True,
            vmem_limit_bytes=VMEM_BYTES - 12 * f_rows * width - 2 * t_rows * span),
    )(tokens, cotangent, expert_ids.T, route_weight.T, gate_weight[0], up_weight[0], down_weight[0])
    dx, route, *wide = pl.pallas_call(
        publish,
        out_shape=tuple(jax.ShapeDtypeStruct(v.shape, v.dtype) for v in pieces),
        in_specs=[vmem] * 5,
        out_specs=(any_,) * 5,
        scratch_shapes=[dma((5,))],
        compiler_params=pltpu.CompilerParams(vmem_limit_bytes=1_000_000),
    )(*(pltpu.with_memory_space_constraint(v, pltpu.VMEM) for v in pieces))
    return dx, route.T, *(g[None] for g in wide)


def solution(mesh):
    in_specs = (
        P("ep", None), P("ep", None), P("ep", None), P("ep", None),
        P("ep", "tp", None), P("ep", "tp", None), P("ep", "tp", None),
    )
    out_specs = (
        P("ep", "tp"), P("ep", None), P("ep", "tp", None), P("ep", "tp", None), P("ep", "tp", None),
    )
    return jax.shard_map(
        per_device, mesh=mesh, in_specs=in_specs, out_specs=out_specs, check_vma=False
    )
```

```python
import functools

import jax
import jax.numpy as jnp
from jax import lax
from jax.experimental import pallas as pl
from jax.experimental.pallas import tpu as pltpu
from jax.sharding import PartitionSpec as P

MESH = pl.DeviceIdType.MESH
F32 = jnp.float32
BF16 = jnp.bfloat16
NT = (((1,), (1,)), ((), ()))
TN = (((0,), (0,)), ((), ()))
VMEM_BYTES = 66_900_000


def slices_for(j, bits, count):
    base = j
    for bit in bits:
        base = base - ((j // bit) % 2) * bit
    out = []
    for k in range(count):
        out.append(base + sum(bit for n, bit in enumerate(bits) if (k >> n) & 1))
    return out


def kernel(
    ep, tp, cap, tokens, cotangent, ids_in, probs_in, gate_w, up_w, down_w,
    dx_out, route_out, gate_out, up_out, down_out,
    ids, probs, xin, hot, hot_t, stage, mate_rows, whole, diag, rows, weights, flipped, pw_out, pw_in, grads, part, ta_in, tb_in, z_in,
    r_send, r_in, r_tp, r_mat,
    load_sem, z_send, z_recv, m_send, m_recv, f_send, f_recv, x_send, x_recv, d_send, d_recv,
    w_send, w_recv, t_send, t_recv, p_send, p_recv, pz_send, pz_recv, rs_send, rs_recv,
    rt_send, rt_recv,
):
    e, j = lax.axis_index("ep"), lax.axis_index("tp")
    levels = ep // 2
    lvl, core = e // 2, e % 2
    mate = e + 1 - 2 * core
    t_rows, width = tokens.shape
    span = width // tp
    half = cap // 2
    nb = tp.bit_length() - 1
    lb = levels.bit_length() - 1
    far = 2 * (levels - 1)
    units = far + 2
    crossed = tp == 4 and far > 2
    spread_end = far - 2 if crossed else far - 1
    tile = min(width, 512)

    def xor(a, b):
        out = 0
        for n in range(lb):
            p, q = (a // (1 << n)) % 2, (b // (1 << n)) % 2
            out = out + (p + q - 2 * p * q) * (1 << n)
        return out

    def level_of(u):
        d = u // 2 + 1 + u % 2
        return xor(lvl, jnp.where(d >= levels, 1, d))

    whole_at = units - 3 if far > 2 else units - 1

    def unit_of(w):
        return jnp.where(w == whole_at, units - 1, jnp.where(w > whole_at, w - 1, w))

    def source(w):
        v = unit_of(w)
        u = jnp.maximum(v - 2, 0)
        return jnp.where(v == 0, e, jnp.where(v == 1, mate, 2 * level_of(u) + u % 2))

    def blk(s):
        return pl.ds(pl.multiple_of(s * cap, cap), cap)

    def col(s):
        return pl.ds(pl.multiple_of(s * span, span), span)

    def run(first, count):
        return pl.ds(pl.multiple_of(first * span, span), count * span)

    def flip(bit):
        return j + bit * (1 - 2 * ((j // bit) % 2))

    def remote(src, dst, ssem, rsem, de, dt):
        return pltpu.make_async_remote_copy(
            src_ref=src, dst_ref=dst, send_sem=ssem, recv_sem=rsem,
            device_id=(de, dt), device_id_type=MESH)

    small = [
        pltpu.make_async_copy(ids_in, ids, load_sem.at[5]),
        pltpu.make_async_copy(probs_in, probs, load_sem.at[6]),
    ]
    loads = [
        pltpu.make_async_copy(tokens, xin.at[0], load_sem.at[0]),
        pltpu.make_async_copy(cotangent, xin.at[1], load_sem.at[1]),
        pltpu.make_async_copy(gate_w, weights.at[0], load_sem.at[2]),
        pltpu.make_async_copy(up_w, weights.at[1], load_sem.at[3]),
        pltpu.make_async_copy(down_w, weights.at[2], load_sem.at[4]),
    ]
    for copy in small + loads:
        copy.start()
    barrier = pltpu.get_barrier_semaphore()

    def greet(n, _):
        pl.semaphore_signal(barrier, inc=1, device_id=(lax.rem(e + n, ep), j), device_id_type=MESH)
        return 0

    def greet_tp(n, _):
        pl.semaphore_signal(barrier, inc=1, device_id=(e, lax.rem(j + n, tp)), device_id_type=MESH)
        return 0

    lax.fori_loop(1, ep, greet, 0)
    lax.fori_loop(1, tp, greet_tp, 0)

    def z_copy(a, u, d):
        return remote(stage.at[a, blk(d)], rows.at[a, blk(e), col(j)],
                      z_send, z_recv.at[a, u], d, j)

    def z_wait(a, u, s):
        return remote(stage.at[a, blk(s)], rows.at[a, blk(s), col(j)],
                      z_send, z_recv.at[a, u], s, j)

    def m_copy(s):
        return remote(mate_rows, rows.at[:, blk(s)], m_send, m_recv, mate, j)

    def full_copy(c, s, d):
        return remote(whole.at[c], rows.at[:, blk(s)], f_send, f_recv, d, j)

    def cross_copy(bit, s, receive):
        peer = flip(bit)
        ref = rows.at[:, blk(s), col(peer if receive else j)]
        return remote(ref, ref, x_send, x_recv.at[bit - 1], e, peer)

    def diag_copy(c, s, d):
        return remote(diag.at[c], rows.at[:, blk(s), col(tp - 1 - j)], d_send, d_recv, d, j)

    def w_copy(d, s):
        return remote(pw_out.at[d], pw_in.at[s], w_send, w_recv.at[0], d, j)

    def w_mate(s):
        return remote(pw_out.at[mate], pw_in.at[s], w_send, w_recv.at[1], mate, j)

    def gather_step(a, u, s, n):
        peer = flip(1 << n if a == 0 else tp >> (n + 1))
        if a == 0:
            ref = rows.at[a, blk(s), run(j - j % (1 << n), 1 << n)]
            return [remote(ref, ref, t_send, t_recv.at[a, u, n], e, peer)]
        copies = []
        for sid in slices_for(j, [tp >> (i + 1) for i in range(n)], 1 << n):
            ref = rows.at[a, blk(s), col(sid)]
            copies.append(remote(ref, ref, t_send, t_recv.at[a, u, n], e, peer))
        return copies

    def gather_wait(a, u, s, n):
        ref = rows.at[a, blk(s), run(0, 1 << n)]
        remote(ref, ref, t_send, t_recv.at[a, u, n], e, flip(1)).wait_recv()

    def scatter_step(w, s, n):
        base, count = tp - (tp >> n), tp >> (n + 1)
        copies = []
        for k in range(count):
            peer = flip(1 << n)
            bits = [1 << i for i in range(n + 1, nb)]
            mine = part.at[s, :half, col(slices_for(j, bits, count)[k])]
            src = part.at[s, :half, col(slices_for(peer, bits, count)[k])]
            got = tb_in.at[s, base + k]
            copies.append((remote(src, got, p_send, p_recv.at[w, n], e, peer), mine, got))
        peer = flip(count)
        mine = part.at[s, half:, run(j - j % count, count)]
        src = part.at[s, half:, run(peer - peer % count, count)]
        got = ta_in.at[s, :, base * span:(base + count) * span]
        copies.append((remote(src, got, p_send, p_recv.at[w, n], e, peer), mine, got))
        return copies

    def scatter_wait(w, n):
        ref = part.at[0, :, run(0, tp >> (n + 1))]
        remote(ref, ref, p_send, p_recv.at[w, n], e, flip(1)).wait_recv()

    def pz_copy(d, s):
        return remote(part.at[d, :, col(j)], z_in.at[blk(s)], pz_send, pz_recv, d, j)

    def r_copy(d, s):
        return remote(r_send.at[d], r_in.at[s], rs_send, rs_recv, d, j)

    def send(u, arrays):
        l = level_of(u)
        for a in arrays:
            for c in range(2):
                z_copy(a, u, 2 * l + c).start()

    for copy in small:
        copy.wait()
    idr = ids[...]
    lane_e = lax.broadcasted_iota(jnp.int32, (ep, t_rows), 0)
    first, second = lane_e == idr[0:1], lane_e == idr[1:2]
    mask = jnp.where(first | second, 1.0, 0.0)
    before = jnp.where(
        lax.broadcasted_iota(jnp.int32, (t_rows, t_rows), 0)
        < lax.broadcasted_iota(jnp.int32, (t_rows, t_rows), 1), 1.0, 0.0).astype(BF16)
    rank = jnp.dot(mask.astype(BF16), before, preferred_element_type=F32)
    key = jnp.where(mask > 0.0, rank, -1.0)
    slot = lax.broadcasted_iota(jnp.int32, (cap, t_rows), 0).astype(F32)
    for x in range(ep):
        hot[x * cap:(x + 1) * cap] = jnp.where(key[x:x + 1] == slot, 1.0, 0.0).astype(BF16)

    def select(a):
        stage[a] = jnp.dot(
            hot[...], xin[a, :, col(j)], preferred_element_type=F32).astype(BF16)

    for a in range(2):
        loads[a].wait()
        select(a)

    p = probs[...].astype(F32)
    chosen = (jnp.where(first, p[0:1], 0.0) + jnp.where(second, p[1:2], 0.0)).astype(BF16)
    slot_p = lax.dot_general(chosen, hot[...], NT, preferred_element_type=F32)
    for x in range(ep):
        pw_out[x, :, :cap] = slot_p[x:x + 1, x * cap:(x + 1) * cap]
    pw_in[e] = pw_out[e]

    def w_start(n, _):
        d = lax.rem(e + n, ep)
        @pl.when(d != mate)
        def _():
            w_copy(d, e).start()
        return 0

    pl.semaphore_wait(barrier, ep + tp - 2)
    lax.fori_loop(1, ep, w_start, 0)
    w_mate(e).start()
    if far:
        send(core, (0, 1))
    for a in range(2):
        for n in range(width // tile):
            cs = pl.ds(n * tile, tile)
            mate_rows[a, :, cs] = jnp.dot(
                hot[blk(mate)], xin[a, :, cs], preferred_element_type=F32).astype(BF16)
            rows[a, blk(e), cs] = jnp.dot(
                hot[blk(e)], xin[a, :, cs], preferred_element_type=F32).astype(BF16)
    m_copy(e).start()

    for k in range(3):
        loads[k + 2].wait()
        for n in range(width // tile):
            cs = pl.ds(n * tile, tile)
            flipped[k, cs] = weights[k, :, cs].T

    def source_of(u):
        return 2 * level_of(u) + u % 2

    def arrive(u):
        s = source_of(u)
        for a in range(2):
            z_wait(a, u, s).wait_recv()
            @pl.when(u < spread_end)
            def _():
                for copy in gather_step(a, u, s, 0):
                    copy.start()
        if crossed:
            @pl.when(u == spread_end)
            def _():
                for bit in (1, 2):
                    cross_copy(bit, s, False).start()

    def spread(u, n):
        s = source_of(u)
        for a in range(2):
            gather_wait(a, u, s, n - 1)
            for copy in gather_step(a, u, s, n):
                copy.start()

    def feed(u):
        @pl.when(core == u % 2)
        def _():
            send(u, (0, 1))

    def feed_cross():
        there = 2 * level_of(spread_end)
        for c in range(2):
            for a in range(2):
                diag[c, a] = jnp.dot(
                    hot[blk(there + c)], xin[a, :, col(tp - 1 - j)],
                    preferred_element_type=F32).astype(BF16)
            diag_copy(c, e, there + c).start()

    def feed_whole():
        near = 2 * level_of(far - 1)
        for c in range(2):
            for a in range(2):
                for n in range(width // tile):
                    cs = pl.ds(n * tile, tile)
                    whole[c, a, :, cs] = jnp.dot(
                        hot[blk(near + c)], xin[a, :, cs], preferred_element_type=F32).astype(BF16)
            full_copy(c, e, near + c).start()

    def compute(w):
        s = source(w)
        @pl.when(w == 1)
        def _():
            m_copy(mate).wait_recv()
            w_mate(mate).wait_recv()
        if far:
            @pl.when(w == 2)
            def _():
                some = pw_in.at[pl.ds(0, ep - 2)]
                remote(some, some, w_send, w_recv.at[0], mate, j).wait_recv()
            if crossed:
                @pl.when(w == units - 1)
                def _():
                    for bit in (1, 2):
                        cross_copy(bit, s, True).wait_recv()
                    diag_copy(0, s, s).wait_recv()
            @pl.when(w == whole_at)
            def _():
                full_copy(0, s, s).wait_recv()
            u = unit_of(w) - 2
            @pl.when(jnp.logical_and(w != whole_at, jnp.logical_and(w >= 2, u < spread_end)))
            def _():
                for a in range(2):
                    gather_wait(a, u, s, nb - 1)
        x = rows[0, blk(s), :]
        pre_gate = jnp.dot(x, flipped[0], preferred_element_type=F32)
        pre_up = jnp.dot(x, flipped[1], preferred_element_type=F32)
        back = jnp.dot(rows[1, blk(s), :], flipped[2], preferred_element_type=F32)
        p = jnp.broadcast_to(pw_in[s], (8, t_rows)).T[:cap, 0:1]
        sigma = jax.nn.sigmoid(pre_gate)
        silu = pre_gate * sigma
        hidden = silu * pre_up
        scaled = p * back
        gg = (scaled * pre_up * sigma * (1.0 + pre_gate * (1.0 - sigma))).astype(BF16)
        gu = (scaled * silu).astype(BF16)
        for n in range(width // tile):
            cs = pl.ds(n * tile, tile)
            part[s, :, cs] = (
                jnp.dot(gg, weights[0, :, cs], preferred_element_type=F32)
                + jnp.dot(gu, weights[1, :, cs], preferred_element_type=F32)).astype(BF16)
        for copy, _, _ in scatter_step(w, s, 0):
            copy.start()
        grads[0, blk(s)] = gg
        grads[1, blk(s)] = gu
        grads[2, blk(s)] = (p * hidden).astype(BF16)
        prod = jnp.sum(hidden * back, axis=1, keepdims=True)
        r_send[s, :, :cap] = jnp.broadcast_to(prod, (cap, t_rows)).T[0:1]
        @pl.when(w >= 1)
        def _():
            r_copy(s, e).start()
        @pl.when(w == 0)
        def _():
            r_in[e] = r_send[e]

    def merge(w, n):
        s = source(w)
        scatter_wait(w, n)
        for _, mine, got in scatter_step(w, s, n):
            mine[...] = (mine[...].astype(F32) + got[...].astype(F32)).astype(BF16)
        if n + 1 < nb:
            for copy, _, _ in scatter_step(w, s, n + 1):
                copy.start()
        else:
            @pl.when(w >= 1)
            def _():
                pz_copy(s, e).start()
            @pl.when(w == 0)
            def _():
                z_in[blk(e)] = part[e, :, col(j)]

    outs = (gate_out, up_out, down_out)

    def weight_grad(k):
        left = grads[k].T
        for n in range(width // tile):
            cs = pl.ds(n * tile, tile)
            outs[k][:, cs] = jnp.dot(left, rows[k // 2, :, cs], preferred_element_type=F32)

    def rt_copy(d, s):
        return remote(r_in, r_tp.at[s], rt_send, rt_recv, e, d)

    def rt_start(n, _):
        rt_copy(lax.rem(j + n, tp), j).start()
        return 0


    bulk = units + nb - 3

    def done(t):
        count = jnp.where(t > bulk, units, jnp.clip(t - nb, 2, units))
        return jnp.where(t < 2, jnp.maximum(t, 0), count)

    def span_of(f, low, high):
        def one(w, _):
            f(w)
            return 0

        lax.fori_loop(low, high, one, 0)

    def merges(t, when):
        @pl.when(when)
        def _():
            for n in range(nb - 1, -1, -1):
                late = functools.partial(merge, n=n)
                if n == 0:
                    span_of(late, done(t - 1), done(t))
                else:
                    span_of(late, jnp.minimum(done(t - 2 - n), 2), jnp.minimum(done(t - 1 - n), 2))
                    span_of(late, jnp.maximum(done(t - 1 - n), 2), jnp.maximum(done(t - n), 2))

    def exchange():
        lines = r_in.at[pl.ds(0, ep - 1)]
        remote(lines, lines, rs_send, rs_recv, mate, j).wait()
        lax.fori_loop(1, tp, rt_start, 0)
        r_tp[j] = r_in[...]

    def tick(t, _):
        def stage_of(f, i, low, high):
            @pl.when(jnp.logical_and(i >= low, i < high))
            def _():
                f(i)

        if far:
            stage_of(feed, jnp.where(t > 2, t, 0), 2, far - 1)
            if crossed:
                @pl.when(jnp.logical_and(t == spread_end + 1, core == 0))
                def _():
                    feed_cross()
            @pl.when(jnp.logical_and(t == max(1, far - 3), core == 1))
            def _():
                feed_whole()
        if far > 2:
            @pl.when(t == bulk)
            def _():
                span_of(compute, whole_at, whole_at + 2)
        merges(t, t >= bulk - 1)
        span_of(compute, done(t) + jnp.where(t == bulk, 2, 0) if far > 2 else done(t), done(t + 1))
        if far:
            stage_of(feed, jnp.where(t == 1, 2, 0), 2, far - 1)
            stage_of(arrive, jnp.where(t <= 2, t - 1, -1), 0, far - 1)
        merges(t, t < bulk - 1)
        if far:
            for n in range(1, nb):
                stage_of(functools.partial(spread, n=n), t - 1 - n, 0, spread_end)
            stage_of(arrive, jnp.where(t > 2, t - 1, -1), 0, far - 1)
        return 0

    if far > 2 and nb == 2:
        lax.fori_loop(0, bulk + 1, tick, 0)
        halves, wholes = functools.partial(merge, n=0), functools.partial(merge, n=1)
        last = units - 1
        span_of(halves, last - 2, last)
        span_of(wholes, last - 3, last - 2)
        span_of(halves, last, units)
        span_of(wholes, last - 1, last)
        span_of(wholes, last - 2, last - 1)
        span_of(wholes, last, units)
        exchange()
    else:
        lax.fori_loop(0, units + 2 * nb - 2, tick, 0)
        exchange()
    for k in range(0, 3):
        weight_grad(k)
    hot_t[...] = hot[...].T
    lines = r_tp.at[pl.ds(0, tp - 1)]
    remote(lines, lines, rt_send, rt_recv, e, flip(1)).wait()
    for x in range(ep):
        total = r_tp[0, x]
        for i in range(1, tp):
            total = total + r_tp[i, x]
        r_mat[x:x + 1, :cap] = total[:, :cap]
    sums = r_mat[...].T
    found = [jnp.zeros((1, t_rows), F32) for _ in range(2)]
    for x in range(ep):
        value = jnp.sum(
            hot[x * cap:(x + 1) * cap].astype(F32) * sums[:cap, x:x + 1], axis=0, keepdims=True)
        found = [f + jnp.where(idr[k:k + 1] == x, value, 0.0) for k, f in enumerate(found)]
    for k in range(2):
        route_out[k:k + 1] = found[k]

    lines = pw_out.at[pl.ds(0, ep - 1)]
    remote(lines, lines, w_send, w_recv.at[0], mate, j).wait_send()
    m_copy(e).wait_send()
    if far:
        @pl.when(core == 0)
        def _():
            sent = stage.at[:, :far * cap]
            remote(sent, sent, z_send, z_recv.at[0, 0], mate, j).wait_send()
            if crossed:
                remote(diag, diag, d_send, d_recv, mate, j).wait_send()
        @pl.when(core == 1)
        def _():
            if far > 2:
                sent = stage.at[:, :(far - 2) * cap]
                remote(sent, sent, z_send, z_recv.at[0, 0], mate, j).wait_send()
            remote(whole, whole, f_send, f_recv, mate, j).wait_send()
        if crossed:
            sent = rows.at[:, :cap, :2 * span]
            remote(sent, sent, x_send, x_recv.at[0], e, flip(1)).wait_send()
        if spread_end:
            sent = rows.at[:, :spread_end * cap, :(tp - 1) * span]
            remote(sent, sent, t_send, t_recv.at[0, 0, 0], e, flip(1)).wait_send()
    sent = part.at[:, :, :(tp - 1) * span]
    remote(sent, sent, p_send, p_recv.at[0, 0], e, flip(1)).wait_send()
    sent = z_in.at[:(ep - 1) * cap]
    remote(sent, sent, pz_send, pz_recv, mate, j).wait()
    dx_out[...] = jnp.dot(hot_t[...], z_in[...], preferred_element_type=F32).astype(BF16)


def publish(*refs):
    srcs, dsts, sem = refs[:5], refs[5:10], refs[10]
    copies = [pltpu.make_async_copy(srcs[k], dsts[k], sem.at[k]) for k in (2, 3, 4, 0, 1)]
    for copy in copies:
        copy.start()
    for copy in copies:
        copy.wait()


def per_device(tokens, cotangent, expert_ids, route_weight, gate_weight, up_weight, down_weight):
    ep, tp = lax.axis_size("ep"), lax.axis_size("tp")
    t_rows, width = tokens.shape
    top = expert_ids.shape[1]
    _, f_rows, _ = gate_weight.shape
    cap = min(t_rows, 2 * top * t_rows // ep)
    span = width // tp
    nb = tp.bit_length() - 1
    any_, vmem = pl.BlockSpec(memory_space=pl.ANY), pl.BlockSpec(memory_space=pltpu.VMEM)
    dma = pltpu.SemaphoreType.DMA
    big = pltpu.VMEM((f_rows, width), F32)
    scratch = [
        pltpu.VMEM(expert_ids.shape[::-1], jnp.int32),
        pltpu.VMEM(route_weight.shape[::-1], route_weight.dtype),
        pltpu.VMEM((2, t_rows, width), BF16),
        pltpu.VMEM((ep * cap, t_rows), BF16),
        pltpu.VMEM((t_rows, ep * cap), BF16),
        pltpu.VMEM((2, ep * cap, span), BF16),
        pltpu.VMEM((2, cap, width), BF16),
        pltpu.VMEM((2, 2, cap, width), BF16),
        pltpu.VMEM((2, 2, cap, span), BF16),
        pltpu.VMEM((2, ep * cap, width), BF16),
        pltpu.VMEM((3, f_rows, width), BF16),
        pltpu.VMEM((3, width, f_rows), BF16),
        pltpu.VMEM((ep, 1, t_rows), F32),
        pltpu.VMEM((ep, 1, t_rows), F32),
        pltpu.VMEM((3, ep * cap, f_rows), BF16),
        pltpu.VMEM((ep, cap, width), BF16),
        pltpu.VMEM((ep, cap // 2, (tp - 1) * span), BF16),
        pltpu.VMEM((ep, tp - 1, cap // 2, span), BF16),
        pltpu.VMEM((ep * cap, span), BF16),
        pltpu.VMEM((ep, 1, t_rows), F32),
        pltpu.VMEM((ep, 1, t_rows), F32),
        pltpu.VMEM((tp, ep, 1, t_rows), F32),
        pltpu.VMEM((ep, t_rows), F32),
        dma((7,)), dma(()), dma((2, max(ep - 3, 1))), dma(()), dma(()), dma(()), dma(()),
        dma(()), dma((2,)), dma(()), dma(()), dma(()), dma((2,)),
        dma(()), dma((2, max(ep - 3, 1), nb)), dma(()), dma((ep, nb)), dma(()), dma(()),
        dma(()), dma(()), dma(()), dma(()),
    ]
    pieces = pl.pallas_call(
        functools.partial(kernel, ep, tp, cap),
        out_shape=(
            pltpu.VMEM((t_rows, span), BF16),
            pltpu.VMEM(expert_ids.shape[::-1], F32), big, big, big),
        in_specs=[any_] * 7,
        out_specs=(vmem,) * 5,
        scratch_shapes=scratch,
        compiler_params=pltpu.CompilerParams(
            collective_id=0, has_side_effects=True,
            vmem_limit_bytes=VMEM_BYTES - 12 * f_rows * width - 2 * t_rows * span),
    )(tokens, cotangent, expert_ids.T, route_weight.T, gate_weight[0], up_weight[0], down_weight[0])
    dx, route, *wide = pl.pallas_call(
        publish,
        out_shape=tuple(jax.ShapeDtypeStruct(v.shape, v.dtype) for v in pieces),
        in_specs=[vmem] * 5,
        out_specs=(any_,) * 5,
        scratch_shapes=[dma((5,))],
        compiler_params=pltpu.CompilerParams(vmem_limit_bytes=1_000_000),
    )(*(pltpu.with_memory_space_constraint(v, pltpu.VMEM) for v in pieces))
    return dx, route.T, *(g[None] for g in wide)


def solution(mesh):
    in_specs = (
        P("ep", None), P("ep", None), P("ep", None), P("ep", None),
        P("ep", "tp", None), P("ep", "tp", None), P("ep", "tp", None),
    )
    out_specs = (
        P("ep", "tp"), P("ep", None), P("ep", "tp", None), P("ep", "tp", None), P("ep", "tp", None),
    )
    return jax.shard_map(
        per_device, mesh=mesh, in_specs=in_specs, out_specs=out_specs, check_vma=False
    )
```

```python
import functools

import jax
import jax.numpy as jnp
from jax import lax
from jax.experimental import pallas as pl
from jax.experimental.pallas import tpu as pltpu
from jax.sharding import PartitionSpec as P

MESH = pl.DeviceIdType.MESH
F32 = jnp.float32
BF16 = jnp.bfloat16
NT = (((1,), (1,)), ((), ()))
TN = (((0,), (0,)), ((), ()))
VMEM_BYTES = 66_900_000


def slices_for(j, bits, count):
    base = j
    for bit in bits:
        base = base - ((j // bit) % 2) * bit
    out = []
    for k in range(count):
        out.append(base + sum(bit for n, bit in enumerate(bits) if (k >> n) & 1))
    return out


def kernel(
    ep, tp, cap, tokens, cotangent, ids_in, probs_in, gate_w, up_w, down_w,
    dx_out, route_out, gate_out, up_out, down_out,
    ids, probs, xin, hot, hot_t, stage, mate_rows, whole, diag, rows, weights, flipped, pw_out, pw_in, grads, part, ta_in, tb_in, z_in,
    r_send, r_in, r_tp, r_mat,
    load_sem, z_send, z_recv, m_send, m_recv, f_send, f_recv, x_send, x_recv, d_send, d_recv,
    w_send, w_recv, t_send, t_recv, p_send, p_recv, pz_send, pz_recv, rs_send, rs_recv,
    rt_send, rt_recv,
):
    e, j = lax.axis_index("ep"), lax.axis_index("tp")
    levels = ep // 2
    lvl, core = e // 2, e % 2
    mate = e + 1 - 2 * core
    t_rows, width = tokens.shape
    span = width // tp
    half = cap // 2
    nb = tp.bit_length() - 1
    lb = levels.bit_length() - 1
    far = 2 * (levels - 1)
    units = far + 2
    crossed = tp == 4 and far > 2
    spread_end = far - 2 if crossed else far - 1
    tile = min(width, 512)

    def xor(a, b):
        out = 0
        for n in range(lb):
            p, q = (a // (1 << n)) % 2, (b // (1 << n)) % 2
            out = out + (p + q - 2 * p * q) * (1 << n)
        return out

    def level_of(u):
        d = u // 2 + 1 + u % 2
        return xor(lvl, jnp.where(d >= levels, 1, d))

    whole_at = units - 3 if far > 2 else units - 1

    def unit_of(w):
        return jnp.where(w == whole_at, units - 1, jnp.where(w > whole_at, w - 1, w))

    def source(w):
        v = unit_of(w)
        u = jnp.maximum(v - 2, 0)
        return jnp.where(v == 0, e, jnp.where(v == 1, mate, 2 * level_of(u) + u % 2))

    def blk(s):
        return pl.ds(pl.multiple_of(s * cap, cap), cap)

    def col(s):
        return pl.ds(pl.multiple_of(s * span, span), span)

    def run(first, count):
        return pl.ds(pl.multiple_of(first * span, span), count * span)

    def flip(bit):
        return j + bit * (1 - 2 * ((j // bit) % 2))

    def remote(src, dst, ssem, rsem, de, dt):
        return pltpu.make_async_remote_copy(
            src_ref=src, dst_ref=dst, send_sem=ssem, recv_sem=rsem,
            device_id=(de, dt), device_id_type=MESH)

    small = [
        pltpu.make_async_copy(ids_in, ids, load_sem.at[5]),
        pltpu.make_async_copy(probs_in, probs, load_sem.at[6]),
    ]
    loads = [
        pltpu.make_async_copy(tokens, xin.at[0], load_sem.at[0]),
        pltpu.make_async_copy(cotangent, xin.at[1], load_sem.at[1]),
        pltpu.make_async_copy(gate_w, weights.at[0], load_sem.at[2]),
        pltpu.make_async_copy(up_w, weights.at[1], load_sem.at[3]),
        pltpu.make_async_copy(down_w, weights.at[2], load_sem.at[4]),
    ]
    for copy in small + loads:
        copy.start()
    barrier = pltpu.get_barrier_semaphore()

    def greet(n, _):
        pl.semaphore_signal(barrier, inc=1, device_id=(lax.rem(e + n, ep), j), device_id_type=MESH)
        return 0

    def greet_tp(n, _):
        pl.semaphore_signal(barrier, inc=1, device_id=(e, lax.rem(j + n, tp)), device_id_type=MESH)
        return 0

    lax.fori_loop(1, ep, greet, 0)
    lax.fori_loop(1, tp, greet_tp, 0)

    def z_copy(a, u, d):
        return remote(stage.at[a, blk(d)], rows.at[a, blk(e), col(j)],
                      z_send, z_recv.at[a, u], d, j)

    def z_wait(a, u, s):
        return remote(stage.at[a, blk(s)], rows.at[a, blk(s), col(j)],
                      z_send, z_recv.at[a, u], s, j)

    def m_copy(s):
        return remote(mate_rows, rows.at[:, blk(s)], m_send, m_recv, mate, j)

    def full_copy(c, s, d):
        return remote(whole.at[c], rows.at[:, blk(s)], f_send, f_recv, d, j)

    def cross_copy(bit, s, receive):
        peer = flip(bit)
        ref = rows.at[:, blk(s), col(peer if receive else j)]
        return remote(ref, ref, x_send, x_recv.at[bit - 1], e, peer)

    def diag_copy(c, s, d):
        return remote(diag.at[c], rows.at[:, blk(s), col(tp - 1 - j)], d_send, d_recv, d, j)

    def w_copy(d, s):
        return remote(pw_out.at[d], pw_in.at[s], w_send, w_recv.at[0], d, j)

    def w_mate(s):
        return remote(pw_out.at[mate], pw_in.at[s], w_send, w_recv.at[1], mate, j)

    def gather_step(a, u, s, n):
        peer = flip(1 << n if a == 0 else tp >> (n + 1))
        if a == 0:
            ref = rows.at[a, blk(s), run(j - j % (1 << n), 1 << n)]
            return [remote(ref, ref, t_send, t_recv.at[a, u, n], e, peer)]
        copies = []
        for sid in slices_for(j, [tp >> (i + 1) for i in range(n)], 1 << n):
            ref = rows.at[a, blk(s), col(sid)]
            copies.append(remote(ref, ref, t_send, t_recv.at[a, u, n], e, peer))
        return copies

    def gather_wait(a, u, s, n):
        ref = rows.at[a, blk(s), run(0, 1 << n)]
        remote(ref, ref, t_send, t_recv.at[a, u, n], e, flip(1)).wait_recv()

    def scatter_step(w, s, n):
        base, count = tp - (tp >> n), tp >> (n + 1)
        copies = []
        for k in range(count):
            peer = flip(1 << n)
            bits = [1 << i for i in range(n + 1, nb)]
            mine = part.at[s, :half, col(slices_for(j, bits, count)[k])]
            src = part.at[s, :half, col(slices_for(peer, bits, count)[k])]
            got = tb_in.at[s, base + k]
            copies.append((remote(src, got, p_send, p_recv.at[w, n], e, peer), mine, got))
        peer = flip(count)
        mine = part.at[s, half:, run(j - j % count, count)]
        src = part.at[s, half:, run(peer - peer % count, count)]
        got = ta_in.at[s, :, base * span:(base + count) * span]
        copies.append((remote(src, got, p_send, p_recv.at[w, n], e, peer), mine, got))
        return copies

    def scatter_wait(w, n):
        ref = part.at[0, :, run(0, tp >> (n + 1))]
        remote(ref, ref, p_send, p_recv.at[w, n], e, flip(1)).wait_recv()

    def pz_copy(d, s):
        return remote(part.at[d, :, col(j)], z_in.at[blk(s)], pz_send, pz_recv, d, j)

    def r_copy(d, s):
        return remote(r_send.at[d], r_in.at[s], rs_send, rs_recv, d, j)

    def send(u, arrays):
        l = level_of(u)
        for a in arrays:
            for c in range(2):
                z_copy(a, u, 2 * l + c).start()

    for copy in small:
        copy.wait()
    idr = ids[...]
    lane_e = lax.broadcasted_iota(jnp.int32, (ep, t_rows), 0)
    first, second = lane_e == idr[0:1], lane_e == idr[1:2]
    mask = jnp.where(first | second, 1.0, 0.0)
    before = jnp.where(
        lax.broadcasted_iota(jnp.int32, (t_rows, t_rows), 0)
        < lax.broadcasted_iota(jnp.int32, (t_rows, t_rows), 1), 1.0, 0.0).astype(BF16)
    rank = jnp.dot(mask.astype(BF16), before, preferred_element_type=F32)
    key = jnp.where(mask > 0.0, rank, -1.0)
    slot = lax.broadcasted_iota(jnp.int32, (cap, t_rows), 0).astype(F32)
    for x in range(ep):
        hot[x * cap:(x + 1) * cap] = jnp.where(key[x:x + 1] == slot, 1.0, 0.0).astype(BF16)

    def select(a):
        stage[a] = jnp.dot(
            hot[...], xin[a, :, col(j)], preferred_element_type=F32).astype(BF16)

    for a in range(2):
        loads[a].wait()
        select(a)

    p = probs[...].astype(F32)
    chosen = (jnp.where(first, p[0:1], 0.0) + jnp.where(second, p[1:2], 0.0)).astype(BF16)
    slot_p = lax.dot_general(chosen, hot[...], NT, preferred_element_type=F32)
    for x in range(ep):
        pw_out[x, :, :cap] = slot_p[x:x + 1, x * cap:(x + 1) * cap]
    pw_in[e] = pw_out[e]

    def w_start(n, _):
        d = lax.rem(e + n, ep)
        @pl.when(d != mate)
        def _():
            w_copy(d, e).start()
        return 0

    pl.semaphore_wait(barrier, ep + tp - 2)
    lax.fori_loop(1, ep, w_start, 0)
    w_mate(e).start()
    if far:
        send(core, (0, 1))
    for a in range(2):
        for n in range(width // tile):
            cs = pl.ds(n * tile, tile)
            mate_rows[a, :, cs] = jnp.dot(
                hot[blk(mate)], xin[a, :, cs], preferred_element_type=F32).astype(BF16)
    m_copy(e).start()
    for a in range(2):
        for n in range(width // tile):
            cs = pl.ds(n * tile, tile)
            rows[a, blk(e), cs] = jnp.dot(
                hot[blk(e)], xin[a, :, cs], preferred_element_type=F32).astype(BF16)

    for k in range(3):
        loads[k + 2].wait()
        for n in range(width // tile):
            cs = pl.ds(n * tile, tile)
            flipped[k, cs] = weights[k, :, cs].T

    def source_of(u):
        return 2 * level_of(u) + u % 2

    def arrive(u):
        s = source_of(u)
        for a in range(2):
            z_wait(a, u, s).wait_recv()
            @pl.when(u < spread_end)
            def _():
                for copy in gather_step(a, u, s, 0):
                    copy.start()
        if crossed:
            @pl.when(u == spread_end)
            def _():
                for bit in (1, 2):
                    cross_copy(bit, s, False).start()

    def spread(u, n):
        s = source_of(u)
        for a in range(2):
            gather_wait(a, u, s, n - 1)
            for copy in gather_step(a, u, s, n):
                copy.start()

    def feed(u):
        @pl.when(core == u % 2)
        def _():
            send(u, (0, 1))

    def feed_cross():
        there = 2 * level_of(spread_end)
        for c in range(2):
            for a in range(2):
                diag[c, a] = jnp.dot(
                    hot[blk(there + c)], xin[a, :, col(tp - 1 - j)],
                    preferred_element_type=F32).astype(BF16)
            diag_copy(c, e, there + c).start()

    def feed_whole():
        near = 2 * level_of(far - 1)
        for c in range(2):
            for a in range(2):
                for n in range(width // tile):
                    cs = pl.ds(n * tile, tile)
                    whole[c, a, :, cs] = jnp.dot(
                        hot[blk(near + c)], xin[a, :, cs], preferred_element_type=F32).astype(BF16)
            full_copy(c, e, near + c).start()

    def compute(w):
        s = source(w)
        @pl.when(w == 1)
        def _():
            m_copy(mate).wait_recv()
            w_mate(mate).wait_recv()
        if far:
            @pl.when(w == 2)
            def _():
                some = pw_in.at[pl.ds(0, ep - 2)]
                remote(some, some, w_send, w_recv.at[0], mate, j).wait_recv()
            if crossed:
                @pl.when(w == units - 1)
                def _():
                    for bit in (1, 2):
                        cross_copy(bit, s, True).wait_recv()
                    diag_copy(0, s, s).wait_recv()
            @pl.when(w == whole_at)
            def _():
                full_copy(0, s, s).wait_recv()
            u = unit_of(w) - 2
            @pl.when(jnp.logical_and(w != whole_at, jnp.logical_and(w >= 2, u < spread_end)))
            def _():
                for a in range(2):
                    gather_wait(a, u, s, nb - 1)
        x = rows[0, blk(s), :]
        pre_gate = jnp.dot(x, flipped[0], preferred_element_type=F32)
        pre_up = jnp.dot(x, flipped[1], preferred_element_type=F32)
        back = jnp.dot(rows[1, blk(s), :], flipped[2], preferred_element_type=F32)
        p = jnp.broadcast_to(pw_in[s], (8, t_rows)).T[:cap, 0:1]
        sigma = jax.nn.sigmoid(pre_gate)
        silu = pre_gate * sigma
        hidden = silu * pre_up
        scaled = p * back
        gg = (scaled * pre_up * sigma * (1.0 + pre_gate * (1.0 - sigma))).astype(BF16)
        gu = (scaled * silu).astype(BF16)
        for n in range(width // tile):
            cs = pl.ds(n * tile, tile)
            part[s, :, cs] = (
                jnp.dot(gg, weights[0, :, cs], preferred_element_type=F32)
                + jnp.dot(gu, weights[1, :, cs], preferred_element_type=F32)).astype(BF16)
        for copy, _, _ in scatter_step(w, s, 0):
            copy.start()
        grads[0, blk(s)] = gg
        grads[1, blk(s)] = gu
        grads[2, blk(s)] = (p * hidden).astype(BF16)
        prod = jnp.sum(hidden * back, axis=1, keepdims=True)
        r_send[s, :, :cap] = jnp.broadcast_to(prod, (cap, t_rows)).T[0:1]
        @pl.when(w >= 1)
        def _():
            r_copy(s, e).start()
        @pl.when(w == 0)
        def _():
            r_in[e] = r_send[e]

    def merge(w, n):
        s = source(w)
        scatter_wait(w, n)
        for _, mine, got in scatter_step(w, s, n):
            mine[...] = (mine[...].astype(F32) + got[...].astype(F32)).astype(BF16)
        if n + 1 < nb:
            for copy, _, _ in scatter_step(w, s, n + 1):
                copy.start()
        else:
            @pl.when(w >= 1)
            def _():
                pz_copy(s, e).start()
            @pl.when(w == 0)
            def _():
                z_in[blk(e)] = part[e, :, col(j)]

    outs = (gate_out, up_out, down_out)

    def weight_grad(k):
        left = grads[k].T
        for n in range(width // tile):
            cs = pl.ds(n * tile, tile)
            outs[k][:, cs] = jnp.dot(left, rows[k // 2, :, cs], preferred_element_type=F32)

    def rt_copy(d, s):
        return remote(r_in, r_tp.at[s], rt_send, rt_recv, e, d)

    def rt_start(n, _):
        rt_copy(lax.rem(j + n, tp), j).start()
        return 0


    bulk = units + nb - 3

    def done(t):
        count = jnp.where(t > bulk, units, jnp.clip(t - nb, 2, units))
        return jnp.where(t < 2, jnp.maximum(t, 0), count)

    def span_of(f, low, high):
        def one(w, _):
            f(w)
            return 0

        lax.fori_loop(low, high, one, 0)

    def merges(t, when):
        @pl.when(when)
        def _():
            for n in range(nb - 1, -1, -1):
                late = functools.partial(merge, n=n)
                if n == 0:
                    span_of(late, done(t - 1), done(t))
                else:
                    span_of(late, jnp.minimum(done(t - 2 - n), 2), jnp.minimum(done(t - 1 - n), 2))
                    span_of(late, jnp.maximum(done(t - 1 - n), 2), jnp.maximum(done(t - n), 2))

    def exchange():
        lines = r_in.at[pl.ds(0, ep - 1)]
        remote(lines, lines, rs_send, rs_recv, mate, j).wait()
        lax.fori_loop(1, tp, rt_start, 0)
        r_tp[j] = r_in[...]

    def tick(t, _):
        def stage_of(f, i, low, high):
            @pl.when(jnp.logical_and(i >= low, i < high))
            def _():
                f(i)

        if far:
            stage_of(feed, jnp.where(t > 2, t, 0), 2, far - 1)
            if crossed:
                @pl.when(jnp.logical_and(t == spread_end + 1, core == 0))
                def _():
                    feed_cross()
            @pl.when(jnp.logical_and(t == max(1, far - 3), core == 1))
            def _():
                feed_whole()
        if far > 2:
            @pl.when(t == bulk)
            def _():
                span_of(compute, whole_at, whole_at + 2)
        merges(t, t >= bulk - 1)
        span_of(compute, done(t) + jnp.where(t == bulk, 2, 0) if far > 2 else done(t), done(t + 1))
        if far:
            stage_of(feed, jnp.where(t == 1, 2, 0), 2, far - 1)
            stage_of(arrive, jnp.where(t <= 2, t - 1, -1), 0, far - 1)
        merges(t, t < bulk - 1)
        if far:
            for n in range(1, nb):
                stage_of(functools.partial(spread, n=n), t - 1 - n, 0, spread_end)
            stage_of(arrive, jnp.where(t > 2, t - 1, -1), 0, far - 1)
        return 0

    if far > 2 and nb == 2:
        lax.fori_loop(0, bulk + 1, tick, 0)
        halves, wholes = functools.partial(merge, n=0), functools.partial(merge, n=1)
        last = units - 1
        span_of(halves, last - 2, last)
        span_of(wholes, last - 3, last - 2)
        span_of(halves, last, units)
        span_of(wholes, last - 1, last)
        span_of(wholes, last - 2, last - 1)
        span_of(wholes, last, units)
        exchange()
    else:
        lax.fori_loop(0, units + 2 * nb - 2, tick, 0)
        exchange()
    for k in range(0, 3):
        weight_grad(k)
    hot_t[...] = hot[...].T
    lines = r_tp.at[pl.ds(0, tp - 1)]
    remote(lines, lines, rt_send, rt_recv, e, flip(1)).wait()
    for x in range(ep):
        total = r_tp[0, x]
        for i in range(1, tp):
            total = total + r_tp[i, x]
        r_mat[x:x + 1, :cap] = total[:, :cap]
    sums = r_mat[...].T
    found = [jnp.zeros((1, t_rows), F32) for _ in range(2)]
    for x in range(ep):
        value = jnp.sum(
            hot[x * cap:(x + 1) * cap].astype(F32) * sums[:cap, x:x + 1], axis=0, keepdims=True)
        found = [f + jnp.where(idr[k:k + 1] == x, value, 0.0) for k, f in enumerate(found)]
    for k in range(2):
        route_out[k:k + 1] = found[k]

    lines = pw_out.at[pl.ds(0, ep - 1)]
    remote(lines, lines, w_send, w_recv.at[0], mate, j).wait_send()
    m_copy(e).wait_send()
    if far:
        @pl.when(core == 0)
        def _():
            sent = stage.at[:, :far * cap]
            remote(sent, sent, z_send, z_recv.at[0, 0], mate, j).wait_send()
            if crossed:
                remote(diag, diag, d_send, d_recv, mate, j).wait_send()
        @pl.when(core == 1)
        def _():
            if far > 2:
                sent = stage.at[:, :(far - 2) * cap]
                remote(sent, sent, z_send, z_recv.at[0, 0], mate, j).wait_send()
            remote(whole, whole, f_send, f_recv, mate, j).wait_send()
        if crossed:
            sent = rows.at[:, :cap, :2 * span]
            remote(sent, sent, x_send, x_recv.at[0], e, flip(1)).wait_send()
        if spread_end:
            sent = rows.at[:, :spread_end * cap, :(tp - 1) * span]
            remote(sent, sent, t_send, t_recv.at[0, 0, 0], e, flip(1)).wait_send()
    sent = part.at[:, :, :(tp - 1) * span]
    remote(sent, sent, p_send, p_recv.at[0, 0], e, flip(1)).wait_send()
    sent = z_in.at[:(ep - 1) * cap]
    remote(sent, sent, pz_send, pz_recv, mate, j).wait()
    dx_out[...] = jnp.dot(hot_t[...], z_in[...], preferred_element_type=F32).astype(BF16)


def publish(*refs):
    srcs, dsts, sem = refs[:5], refs[5:10], refs[10]
    copies = [pltpu.make_async_copy(srcs[k], dsts[k], sem.at[k]) for k in (2, 3, 4, 0, 1)]
    for copy in copies:
        copy.start()
    for copy in copies:
        copy.wait()


def per_device(tokens, cotangent, expert_ids, route_weight, gate_weight, up_weight, down_weight):
    ep, tp = lax.axis_size("ep"), lax.axis_size("tp")
    t_rows, width = tokens.shape
    top = expert_ids.shape[1]
    _, f_rows, _ = gate_weight.shape
    cap = min(t_rows, 2 * top * t_rows // ep)
    span = width // tp
    nb = tp.bit_length() - 1
    any_, vmem = pl.BlockSpec(memory_space=pl.ANY), pl.BlockSpec(memory_space=pltpu.VMEM)
    dma = pltpu.SemaphoreType.DMA
    big = pltpu.VMEM((f_rows, width), F32)
    scratch = [
        pltpu.VMEM(expert_ids.shape[::-1], jnp.int32),
        pltpu.VMEM(route_weight.shape[::-1], route_weight.dtype),
        pltpu.VMEM((2, t_rows, width), BF16),
        pltpu.VMEM((ep * cap, t_rows), BF16),
        pltpu.VMEM((t_rows, ep * cap), BF16),
        pltpu.VMEM((2, ep * cap, span), BF16),
        pltpu.VMEM((2, cap, width), BF16),
        pltpu.VMEM((2, 2, cap, width), BF16),
        pltpu.VMEM((2, 2, cap, span), BF16),
        pltpu.VMEM((2, ep * cap, width), BF16),
        pltpu.VMEM((3, f_rows, width), BF16),
        pltpu.VMEM((3, width, f_rows), BF16),
        pltpu.VMEM((ep, 1, t_rows), F32),
        pltpu.VMEM((ep, 1, t_rows), F32),
        pltpu.VMEM((3, ep * cap, f_rows), BF16),
        pltpu.VMEM((ep, cap, width), BF16),
        pltpu.VMEM((ep, cap // 2, (tp - 1) * span), BF16),
        pltpu.VMEM((ep, tp - 1, cap // 2, span), BF16),
        pltpu.VMEM((ep * cap, span), BF16),
        pltpu.VMEM((ep, 1, t_rows), F32),
        pltpu.VMEM((ep, 1, t_rows), F32),
        pltpu.VMEM((tp, ep, 1, t_rows), F32),
        pltpu.VMEM((ep, t_rows), F32),
        dma((7,)), dma(()), dma((2, max(ep - 3, 1))), dma(()), dma(()), dma(()), dma(()),
        dma(()), dma((2,)), dma(()), dma(()), dma(()), dma((2,)),
        dma(()), dma((2, max(ep - 3, 1), nb)), dma(()), dma((ep, nb)), dma(()), dma(()),
        dma(()), dma(()), dma(()), dma(()),
    ]
    pieces = pl.pallas_call(
        functools.partial(kernel, ep, tp, cap),
        out_shape=(
            pltpu.VMEM((t_rows, span), BF16),
            pltpu.VMEM(expert_ids.shape[::-1], F32), big, big, big),
        in_specs=[any_] * 7,
        out_specs=(vmem,) * 5,
        scratch_shapes=scratch,
        compiler_params=pltpu.CompilerParams(
            collective_id=0, has_side_effects=True,
            vmem_limit_bytes=VMEM_BYTES - 12 * f_rows * width - 2 * t_rows * span),
    )(tokens, cotangent, expert_ids.T, route_weight.T, gate_weight[0], up_weight[0], down_weight[0])
    dx, route, *wide = pl.pallas_call(
        publish,
        out_shape=tuple(jax.ShapeDtypeStruct(v.shape, v.dtype) for v in pieces),
        in_specs=[vmem] * 5,
        out_specs=(any_,) * 5,
        scratch_shapes=[dma((5,))],
        compiler_params=pltpu.CompilerParams(vmem_limit_bytes=1_000_000),
    )(*(pltpu.with_memory_space_constraint(v, pltpu.VMEM) for v in pieces))
    return dx, route.T, *(g[None] for g in wide)


def solution(mesh):
    in_specs = (
        P("ep", None), P("ep", None), P("ep", None), P("ep", None),
        P("ep", "tp", None), P("ep", "tp", None), P("ep", "tp", None),
    )
    out_specs = (
        P("ep", "tp"), P("ep", None), P("ep", "tp", None), P("ep", "tp", None), P("ep", "tp", None),
    )
    return jax.shard_map(
        per_device, mesh=mesh, in_specs=in_specs, out_specs=out_specs, check_vma=False
    )
```
